512 devices in a mesh: ep: 32 (over z, core), tp: 16 (over y, x).
Axes of the slice: x: 4, y: 4, z: 16, core: 2. Of those that a mesh axis runs over, the one named last changes fastest.
Arguments:
- tokens: bfloat16 [4096, 1024], P('ep', 'tp'), may hold values from -6 to 6
- norm_gain: float32 [1024], replicated, may hold values from 0.1 to 1.9
- gate_weight: bfloat16 [32, 1024, 1024], P('ep', None, 'tp'), may hold values from -0.1875 to 0.1875
- up_weight: bfloat16 [32, 1024, 1024], P('ep', None, 'tp'), may hold values from -0.1875 to 0.1875
- down_weight: bfloat16 [32, 1024, 1024], P('ep', None, 'tp'), may hold values from -0.1875 to 0.1875
- expert_ids: int32 [4096, 4], P('ep'), may hold values from 0 to 31, all different within a row; in each aligned block of 128 rows (0 to 127, 128 to 255, ...) at most 32 rows name the same one
- route_weight: float32 [4096, 4], P('ep'), may hold values from 0.2 to 1
Outputs:
- combined: bfloat16 [4096, 1024], P('ep', 'tp')
The draws below stay inside these ranges and needn't reach their ends.
Inputs may be any that keep to these rules, and one draw needn't show every extreme that they name: `expert_ids`: each token names 4 different experts; in each aligned block of 128 tokens no expert is named by more than 32 of them, and in some block one expert is named by exactly 32; every expert is named by some token.
All inputs are finite; a program needn't handle non-finite values.
Results may differ from the reference program's by a relative error of at most 0.0035.
Values may be sent and summed in bfloat16 or wider, within the bound.
No kernel may reach another device: no remote copies, remote signals or barrier semaphores. Data moves between devices by JAX's collectives and lax.ppermute only.
A program may use at most 64 MiB of HBM per device.

```python
import math
import jax
import jax.numpy as jnp
import numpy as np
from jax import lax

D = 1024
FF = 1024
TOPK = 4
TOK_DEV = 128
EXPERTS = 32
TOKENS = 4096
CAP = 32
N_EP = 32


def level_of(key, shape, cuts, low, top_value):
    def one(position, blocks):
        heights = jax.random.uniform(jax.random.fold_in(jax.random.fold_in(key, 6), position), (blocks,), jnp.float32, low / len(cuts), top_value / len(cuts))
        return jnp.repeat(jnp.exp(heights), shape[position] // blocks).reshape((-1,) + (1,) * (len(shape) - position - 1))

    gain = one(*cuts[0])
    for cut in cuts[1:]:
        gain = gain * one(*cut)
    return gain


def deal_out(rng, own, number, rows, amount, top, bound, lean):
    order = jax.random.permutation(rng, amount)
    crowded, usual = shares(amount, rows * top, bound, lean, True), shares(amount, rows * top, bound, lean, False)
    places = jnp.arange(amount)

    def named(sizes, rotation):
        used = int((sizes > 0).sum())
        fixed = max(1, used // 4)
        passed = fixed + (places - fixed + rotation * (used - fixed)) % max(1, amount - fixed)
        return jnp.zeros((amount,), jnp.int32).at[order[jnp.where(places < fixed, places, passed)]].set(jnp.asarray(sizes, jnp.int32))

    sizes = jnp.where(number % 4 == 0, named(crowded, number // 4), named(usual, number - number // 4 - 1))
    mixed = jax.random.permutation(jax.random.fold_in(own, 3), amount)
    giver, taker = mixed[0:amount // 2 * 2:2], mixed[1:amount // 2 * 2:2]
    room = jnp.minimum(sizes[giver] - 1, bound - sizes[taker]) // 2
    room = jnp.where((giver == order[0]) | (taker == order[0]) | (sizes[taker] == 0), 0, jnp.maximum(room, 0))
    passed = jax.random.randint(jax.random.fold_in(own, 4), (amount // 2,), 0, 1 << 20) % (room + 1)
    sizes = sizes.at[giver].add(-passed).at[taker].add(passed)
    members = jnp.searchsorted(jnp.cumsum(sizes), jnp.arange(rows * top), side="right").astype(jnp.int32)
    grid = members.reshape(top, rows).T
    grid = grid[jax.random.permutation(jax.random.fold_in(own, 1), rows)]
    rotation = jax.random.randint(jax.random.fold_in(own, 2), (rows, 1), 0, top)
    return jnp.take_along_axis(grid, (jnp.arange(top)[None, :] + rotation) % top, axis=1)


def shares(number_of, total, most, slope, full):
    weights = [(1 << 20) // math.isqrt(grade ** slope) + 1 for grade in range(1, number_of + 1)]
    largest = most if full else min(most, max(-(-total // number_of), total * weights[0] // sum(weights)))
    least = 1 if total - largest >= number_of - 1 else 0
    given, rest = [largest] + [least] * (number_of - 1), total - largest - least * (number_of - 1)
    while rest > 0:
        free = [i for i in range(1, number_of) if given[i] < largest] or [i for i in range(1, number_of) if given[i] < most]
        pool, left = sum([weights[i] for i in free]), rest
        for i in free:
            extra = min(most - given[i], max(1, left * weights[i] // pool), rest)
            given[i] = given[i] + extra
            rest = rest - extra
    return np.array(given)


def noise(key, shape, scale, most, shards=(), held_as=jnp.bfloat16):
    array = scale * jax.random.normal(key, shape, jnp.float32)
    if shards:
        array = array * level_of(key, shape, shards, -0.22, 0.18)
    return jnp.clip(array, -most, most).astype(held_as)


def setup_inputs(seed: int = 0) -> dict:
    keys = jax.random.split(jax.random.key(seed), 8)
    tokens = noise(keys[0], (TOKENS, D), 1.0, 6.0, ((0, 32), (1, 16)))
    norm_gain = jnp.clip(1.0 + 0.18 * jax.random.normal(keys[1], (D,), jnp.float32), 0.1, 1.9)
    gate_weight = noise(keys[2], (EXPERTS, D, FF), D ** -0.5, 0.1875, ((0, 32), (2, 16)))
    up_weight = noise(keys[3], (EXPERTS, D, FF), D ** -0.5, 0.1875, ((0, 32), (2, 16)))
    down_weight = noise(keys[4], (EXPERTS, FF, D), FF ** -0.5, 0.1875, ((0, 32), (2, 16)))
    expert_ids_keys = jax.random.split(jax.random.fold_in(keys[5], 1), TOKENS // TOK_DEV)
    expert_ids_turns = jax.random.permutation(jax.random.fold_in(keys[5], 3), TOKENS // TOK_DEV)
    expert_ids = jax.vmap(lambda own, number: deal_out(jax.random.fold_in(keys[5], 2), own, number, TOK_DEV, EXPERTS, TOPK, CAP, 2))(expert_ids_keys, expert_ids_turns).reshape((TOKENS, TOPK))
    route_weight = jnp.clip(0.2 + 0.8 * jax.random.uniform(keys[6], (TOKENS, TOPK), jnp.float32) ** level_of(keys[6], (TOKENS, TOPK), ((0, 32),), -0.2, 0.2), 0.2, 1.0)
    return {"tokens": tokens, "norm_gain": norm_gain, "gate_weight": gate_weight, "up_weight": up_weight, "down_weight": down_weight, "expert_ids": expert_ids, "route_weight": route_weight}


epsilon = 1e-06
swish_alpha = 1.702
clamp_limit = 7.0

def rms_normed(values, norm_gain):
    widened = values.astype(jnp.float32)
    scaled = widened * lax.rsqrt(lax.optimization_barrier(jnp.mean(widened * widened, axis=-1, keepdims=True)) + epsilon)
    return (scaled * norm_gain.astype(jnp.float32)).astype(jnp.bfloat16)

def slot_numbers(flat_ids, expert_count):
    selector = (flat_ids[..., None] == jnp.arange(expert_count, dtype=jnp.int32)).astype(jnp.int32)
    before = jnp.cumsum(selector, axis=-2) - selector
    return lax.optimization_barrier(jnp.sum(before * selector, axis=-1)).astype(jnp.int32)

def clamped_units(row_block, w_gate, w_up, w_down):
    gate_pre = jnp.dot(row_block, w_gate, preferred_element_type=jnp.float32)
    up_pre = jnp.dot(row_block, w_up, preferred_element_type=jnp.float32)
    gate_pre = jnp.minimum(gate_pre, clamp_limit)
    up_pre = jnp.clip(up_pre, -clamp_limit, clamp_limit)
    hidden = ((up_pre + 1.0) * gate_pre * jax.nn.sigmoid(swish_alpha * gate_pre)).astype(jnp.bfloat16)
    return jnp.dot(hidden, w_down, preferred_element_type=jnp.float32).astype(jnp.bfloat16)

def reference(tokens, norm_gain, gate_weight, up_weight, down_weight, expert_ids, route_weight):
    normed = rms_normed(tokens, norm_gain)
    assigned = TOK_DEV * TOPK
    flat_ids = expert_ids.reshape(N_EP, assigned).astype(jnp.int32)
    slot_index = slot_numbers(flat_ids, EXPERTS)
    source = jnp.broadcast_to(jnp.arange(N_EP, dtype=jnp.int32)[:, None], (N_EP, assigned))
    owner_token = source * TOK_DEV + jnp.arange(assigned, dtype=jnp.int32)[None, :] // TOPK
    slot_table = jnp.full((EXPERTS, N_EP, CAP), TOKENS, jnp.int32).at[flat_ids, source, slot_index].set(owner_token)
    padded = jnp.concatenate([normed, jnp.zeros((1, D), jnp.bfloat16)], axis=0)

    def one_expert(packed):
        index_table, w_gate, w_up, w_down = packed
        return clamped_units(padded[index_table.reshape(-1)], w_gate, w_up, w_down)
    results = lax.map(one_expert, (slot_table, gate_weight, up_weight, down_weight))
    flat_results = results.reshape(EXPERTS * N_EP * CAP, D)
    locator = ((flat_ids * N_EP + source) * CAP + slot_index).reshape(TOKENS, TOPK)
    picked = flat_results[locator].astype(jnp.float32)
    combined = lax.optimization_barrier(jnp.sum(picked * route_weight.astype(jnp.float32)[:, :, None], axis=1))
    return combined.astype(jnp.bfloat16)
```

```python
import jax
import jax.numpy as jnp
from jax import lax
from jax.sharding import Mesh
from jax.sharding import PartitionSpec as P

EP, TY, TX = "ep", "ty", "tx"
TP = (TY, TX)
EPSILON = 1e-06
ALPHA = 1.702
LIMIT = 7.0
BF16, F32 = jnp.bfloat16, jnp.float32


def routed_to(expert_ids, expert_count):
    experts = jnp.arange(expert_count, dtype=jnp.int32)
    picks = expert_ids[:, :, None] == experts
    named = jnp.any(picks, axis=1)
    tok_rows = expert_ids.shape[0]
    earlier = jnp.arange(tok_rows)[:, None] > jnp.arange(tok_rows)[None, :]
    before = jnp.dot(earlier.astype(BF16), named.astype(BF16), preferred_element_type=F32)
    return jnp.sum(jnp.where(picks, before[:, None, :], 0.0), axis=2).astype(jnp.int32)


def body(tokens, norm_gain, gate_weight, up_weight, down_weight, expert_ids, route_weight):
    tok_rows, top = expert_ids.shape
    width = tokens.shape[1]
    full = norm_gain.shape[0]
    ep, ny, nx = lax.axis_size(EP), lax.axis_size(TY), lax.axis_size(TX)
    tp = ny * nx
    units = gate_weight.shape[2]
    half = tok_rows * top // ep
    group = ep // nx * half

    gate_up = jnp.concatenate([gate_weight[0], up_weight[0]], axis=1)
    gate_up = lax.all_to_all(
        jnp.broadcast_to(gate_up, (nx,) + gate_up.shape), TX, 0, 0, tiled=True
    )
    mine = nx * units
    down = down_weight[0].reshape(ny, 2, mine // 2, width)
    down = jnp.transpose(down, (0, 2, 1, 3)).reshape(ny, 1, mine // 2, 2 * width)
    down = jnp.broadcast_to(down, (ny, nx, mine // 2, 2 * width)).reshape(tp, mine // 2, 2 * width)
    down = lax.all_to_all(down, TP, 0, 0, tiled=True)

    slot = routed_to(expert_ids, ep)
    place = expert_ids * half + slot % half
    high = slot // half
    lanes = jnp.arange(ep * half, dtype=jnp.int32)
    hits = place[:, :, None] == lanes
    sel = [jnp.any(hits & (high == h)[:, :, None], axis=1).astype(BF16) for h in (0, 1)]
    sent = jnp.concatenate(
        [jnp.einsum("tp,tf->pf", s, tokens, preferred_element_type=F32) for s in sel], axis=1
    ).astype(BF16)
    got = lax.all_to_all(sent.reshape(ep, half, 2 * width), EP, 0, 0, tiled=True)

    got = got.reshape(1, nx, group, 2 * width)
    got = jnp.broadcast_to(got, (ny, nx, group, 2 * width)).reshape(tp, group, 2 * width)
    got = lax.all_to_all(got, TP, 0, 0, tiled=True)
    rows = jnp.transpose(got.reshape(tp, group, 2, width), (2, 1, 0, 3)).reshape(2 * group, full)
    rows = rows.astype(F32)
    inverse = lax.rsqrt(jnp.mean(rows * rows, axis=1, keepdims=True) + EPSILON)
    normed = (rows * inverse * norm_gain.astype(F32)).astype(BF16)
    gate_pre = jnp.einsum("rd,xdf->rxf", normed, gate_up[:, :, :units], preferred_element_type=F32)
    up_pre = jnp.einsum("rd,xdf->rxf", normed, gate_up[:, :, units:], preferred_element_type=F32)
    gate_pre = jnp.minimum(gate_pre, LIMIT)
    up_pre = jnp.clip(up_pre, -LIMIT, LIMIT)
    hidden = ((up_pre + 1.0) * gate_pre * jax.nn.sigmoid(ALPHA * gate_pre)).astype(BF16)
    hidden = hidden.reshape(2 * group, mine)
    w_down = jnp.transpose(down.reshape(tp, mine // 2, 2, width), (2, 1, 0, 3)).reshape(mine, full)
    part = jnp.dot(hidden, w_down, preferred_element_type=F32)
    part = jnp.transpose(part.reshape(2, group, tp, width), (2, 1, 0, 3))
    part = lax.all_to_all(part.reshape(tp, group, 2 * width), TP, 0, 0, tiled=True)
    out = jnp.sum(part.reshape(ny, nx * group, 2 * width), axis=0).astype(BF16)

    back = lax.all_to_all(out.reshape(ep, half, 2 * width), EP, 0, 0, tiled=True)
    back = back.reshape(ep * half, 2 * width)
    total = jnp.zeros((tok_rows, width), F32)
    for h in (0, 1):
        mix = jnp.sum(
            jnp.where(hits & (high == h)[:, :, None], route_weight[:, :, None], 0.0), axis=1
        )
        mix_hi = mix.astype(BF16)
        mix_lo = (mix - mix_hi.astype(F32)).astype(BF16)
        piece = back[:, h * width : (h + 1) * width]
        total = total + jnp.dot(mix_hi, piece, preferred_element_type=F32)
        total = total + jnp.dot(mix_lo, piece, preferred_element_type=F32)
    return total.astype(BF16)


def solution(mesh):
    devices = mesh.devices.reshape(mesh.shape["ep"], 4, 4)
    split = Mesh(devices, (EP, TY, TX))
    in_specs = (
        P(EP, TP),
        P(),
        P(EP, None, TP),
        P(EP, None, TP),
        P(EP, None, TP),
        P(EP, None),
        P(EP, None),
    )
    return jax.shard_map(
        body, mesh=split, in_specs=in_specs, out_specs=P(EP, TP), check_vma=False
    )
```

```python
import jax
import jax.numpy as jnp
from jax import lax
from jax.sharding import Mesh
from jax.sharding import PartitionSpec as P

EP, TY, TX = "ep", "ty", "tx"
TP = (TY, TX)
EPSILON = 1e-06
ALPHA = 1.702
LIMIT = 7.0
BF16, F32 = jnp.bfloat16, jnp.float32


def routed_to(expert_ids, expert_count):
    experts = jnp.arange(expert_count, dtype=jnp.int32)
    picks = expert_ids[:, :, None] == experts
    named = jnp.any(picks, axis=1)
    tok_rows = expert_ids.shape[0]
    earlier = jnp.arange(tok_rows)[:, None] > jnp.arange(tok_rows)[None, :]
    before = jnp.dot(earlier.astype(BF16), named.astype(BF16), preferred_element_type=F32)
    return jnp.sum(jnp.where(picks, before[:, None, :], 0.0), axis=2).astype(jnp.int32)


def gathered(shard, axis):
    count = lax.axis_size(axis)
    me = lax.axis_index(axis)
    whole = jnp.zeros((count,) + shard.shape, shard.dtype)
    whole = lax.dynamic_update_slice_in_dim(whole, shard[None], me, 0)
    for hop in range(1, count):
        piece = lax.ppermute(shard, axis, [(i, (i + hop) % count) for i in range(count)])
        whole = lax.dynamic_update_slice_in_dim(whole, piece[None], (me - hop) % count, 0)
    return whole


def body(tokens, norm_gain, gate_weight, up_weight, down_weight, expert_ids, route_weight):
    tok_rows, top = expert_ids.shape
    width = tokens.shape[1]
    full = norm_gain.shape[0]
    ep, ny, nx = lax.axis_size(EP), lax.axis_size(TY), lax.axis_size(TX)
    tp = ny * nx
    units = gate_weight.shape[2]
    half = tok_rows * top // ep
    group = ep // nx * half
    mine = nx * units

    with jax.named_scope("weights"):
        shard = jnp.stack([w[0].T for w in (gate_weight, up_weight, down_weight)])
        weights = gathered(shard, TX)
    w_gate, w_up, w_down = (weights[:, i].reshape(mine, full) for i in range(3))

    slot = routed_to(expert_ids, ep)
    place = expert_ids * half + slot % half
    high = slot // half
    lanes = jnp.arange(ep * half, dtype=jnp.int32)
    hits = place[:, :, None] == lanes
    sel = [jnp.any(hits & (high == h)[:, :, None], axis=1).astype(BF16) for h in (0, 1)]
    sent = jnp.concatenate(
        [jnp.einsum("tp,tf->pf", s, tokens, preferred_element_type=F32) for s in sel], axis=1
    ).astype(BF16)
    got = lax.all_to_all(sent.reshape(ep, half, 2 * width), EP, 0, 0, tiled=True)

    got = got.reshape(1, nx, group, 2 * width)
    got = jnp.broadcast_to(got, (ny, nx, group, 2 * width)).reshape(tp, group, 2 * width)
    got = lax.all_to_all(got, TP, 0, 0, tiled=True)
    rows = jnp.transpose(got.reshape(tp, group, 2, width), (2, 1, 0, 3)).reshape(2 * group, full)
    rows = rows.astype(F32)
    inverse = lax.rsqrt(jnp.mean(rows * rows, axis=1, keepdims=True) + EPSILON)
    normed = (rows * inverse * norm_gain.astype(F32)).astype(BF16)
    gate_pre = jnp.einsum("fd,rd->fr", w_gate, normed, preferred_element_type=F32)
    up_pre = jnp.einsum("fd,rd->fr", w_up, normed, preferred_element_type=F32)
    gate_pre = jnp.minimum(gate_pre, LIMIT)
    up_pre = jnp.clip(up_pre, -LIMIT, LIMIT)
    hidden = ((up_pre + 1.0) * gate_pre * jax.nn.sigmoid(ALPHA * gate_pre)).astype(BF16)

    hidden = jnp.broadcast_to(hidden, (ny,) + hidden.shape)
    hidden = lax.all_to_all(hidden, TY, 0, 0, tiled=True).reshape(full, 2 * group)
    out = jnp.dot(w_down, hidden, preferred_element_type=F32).astype(BF16)
    out = lax.all_to_all(out.reshape(nx, width, 2 * group), TX, 0, 0, tiled=True)
    out = out.reshape(nx, width, 2, ep // nx, half)
    out = jnp.transpose(out, (0, 3, 4, 2, 1)).reshape(ep, half, 2 * width)

    back = lax.all_to_all(out, EP, 0, 0, tiled=True).reshape(ep * half, 2 * width)
    total = jnp.zeros((tok_rows, width), F32)
    for h in (0, 1):
        mix = jnp.sum(
            jnp.where(hits & (high == h)[:, :, None], route_weight[:, :, None], 0.0), axis=1
        )
        first = lax.reduce_precision(mix, 8, 7)
        rest = lax.reduce_precision(mix - first, 8, 7)
        piece = back[:, h * width : (h + 1) * width]
        for part in (first, rest):
            total = total + jnp.dot(part.astype(BF16), piece, preferred_element_type=F32)
    return total.astype(BF16)


def solution(mesh):
    devices = mesh.devices.reshape(mesh.shape["ep"], 4, 4)
    split = Mesh(devices, (EP, TY, TX))
    in_specs = (
        P(EP, TP),
        P(),
        P(EP, None, TP),
        P(EP, None, TP),
        P(EP, None, TP),
        P(EP, None),
        P(EP, None),
    )
    return jax.shard_map(
        body, mesh=split, in_specs=in_specs, out_specs=P(EP, TP), check_vma=False
    )
```

```python
import functools

import jax
import jax.numpy as jnp
from jax import lax
from jax.experimental import pallas as pl
from jax.experimental.pallas import tpu as pltpu
from jax.sharding import Mesh
from jax.sharding import PartitionSpec as P


EP, TY, TX = "ep", "ty", "tx"
TP = (TY, TX)
EPSILON = 1e-06
ALPHA = 1.702
LIMIT = 7.0
BF16, F32, I32 = jnp.bfloat16, jnp.float32, jnp.int32
NT = (((1,), (1,)), ((), ()))


def iota(shape, dim):
    return lax.broadcasted_iota(I32, shape, dim)


def dot(a, b):
    return jnp.dot(a, b, preferred_element_type=F32)


def dot_nt(a, b):
    return lax.dot_general(a, b, NT, preferred_element_type=F32)


def ones_where(mask):
    return jnp.where(mask, 1.0, 0.0).astype(BF16)


def swapped(count, middle, inner):
    outer = count // (middle * inner)
    to, source = iota((count, count), 0), iota((count, count), 1)
    m, o, i = to // (outer * inner), (to // inner) % outer, to % inner
    return ones_where(source == (o * middle + m) * inner + i)


def halves(first, second):
    wide = first.shape[1] // 2
    left = iota(first.shape, 1) < wide
    return (
        jnp.where(left, first, pltpu.roll(second, wide, 1)),
        jnp.where(left, pltpu.roll(first, wide, 1), second),
    )


def prep_kernel(experts, ids_ref, tokens_ref, sent_ref, place_ref):
    top, toks = ids_ref.shape
    count, _ = sent_ref.shape
    half = count // experts
    ids = ids_ref[...]
    expert = iota((experts, toks), 0)
    picks = [expert == ids[k : k + 1] for k in range(top)]
    named = picks[0]
    for pick in picks[1:]:
        named = named | pick
    earlier = ones_where(iota((toks, toks), 0) < iota((toks, toks), 1))
    before = dot(ones_where(named), earlier)
    lane = iota((2 * count, toks), 0)
    hit = None
    for k in range(top):
        slot = jnp.sum(jnp.where(picks[k], before, 0.0), axis=0, keepdims=True).astype(I32)
        high = jnp.where(slot >= half, 1, 0)
        place = ids[k : k + 1] * half + slot - half * high + count * high
        place_ref[k : k + 1] = place
        hit = (lane == place) if hit is None else hit | (lane == place)
    select = ones_where(hit)
    tokens = tokens_ref[...].astype(F32)
    zero = jnp.zeros_like(tokens)
    both = jnp.concatenate(
        [jnp.concatenate([tokens, zero], 1), jnp.concatenate([zero, tokens], 1)], 0
    ).astype(BF16)
    both_select = jnp.concatenate([select[:count], select[count:]], 1)
    sent_ref[...] = dot_nt(both_select, both).astype(BF16)


def mix_kernel(place_ref, weight_ref, first_ref, rest_ref):
    count, toks = first_ref.shape
    lane = iota((count, toks), 0)
    mix = jnp.zeros((count, toks), F32)
    for k in range(place_ref.shape[0]):
        mix = mix + jnp.where(lane == place_ref[k : k + 1], weight_ref[k : k + 1], 0.0)
    first = mix.astype(BF16)
    first_ref[...] = first
    rest_ref[...] = (mix - first.astype(F32)).astype(BF16)


def spread_kernel(got_ref, out_ref):
    count = got_ref.shape[0]
    copies, groups, group, _ = out_ref.shape
    order = swapped(count, groups, 4)
    moved = dot(order, got_ref[...]).astype(BF16)
    for g in range(groups):
        for c in range(copies):
            out_ref[c, g] = moved[g * group : (g + 1) * group]


def up_kernel(rows_ref, gain_ref, weights_ref, out_ref, whole, normed):
    pieces, group, wide = rows_ref.shape
    full = normed.shape[1]
    squares = [jnp.zeros((group, wide), F32) for _ in range(2)]
    for j in range(pieces // 2):
        pair = halves(rows_ref[2 * j].astype(F32), rows_ref[2 * j + 1].astype(F32))
        for h in range(2):
            whole[h * group : (h + 1) * group, j * wide : (j + 1) * wide] = pair[h]
            squares[h] = squares[h] + pair[h] * pair[h]
    for h in range(2):
        mean = jnp.sum(squares[h], axis=1, keepdims=True) / full
        inverse = lax.rsqrt(mean + EPSILON)
        rows = slice(h * group, (h + 1) * group)
        normed[rows] = (whole[rows] * inverse * gain_ref[...]).astype(BF16)
    nx, _, units, _ = weights_ref.shape
    w_gate = weights_ref[:, 0].reshape(nx * units, full)
    w_up = weights_ref[:, 1].reshape(nx * units, full)
    gate = jnp.minimum(dot_nt(normed[...], w_gate), LIMIT)
    up = jnp.clip(dot_nt(normed[...], w_up), -LIMIT, LIMIT)
    hidden = ((up + 1.0) * gate * jax.nn.sigmoid(ALPHA * gate)).astype(BF16)
    for c in range(out_ref.shape[0]):
        out_ref[c] = hidden


def down_kernel(hidden_ref, weights_ref, out_ref):
    ny, rows, units = hidden_ref.shape
    nx, _, width, full = weights_ref.shape
    w_down = weights_ref[:, 2].reshape(nx * width, full)
    total = dot_nt(hidden_ref[0], w_down[:, :units])
    for y in range(1, ny):
        total = total + dot_nt(hidden_ref[y], w_down[:, y * units : (y + 1) * units])
    group = rows // 2
    pieces = []
    for j in range(nx // 2):
        lanes = slice(2 * j * width, 2 * (j + 1) * width)
        pieces += halves(total[:group, lanes], total[group:, lanes])
    stacked = jnp.concatenate(pieces, 0).astype(BF16)
    order = swapped(stacked.shape[0], stacked.shape[0] // (nx * 4), 4)
    out_ref[...] = dot(order, stacked).astype(BF16)


def combine_kernel(back_ref, first_ref, rest_ref, out_ref):
    count = back_ref.shape[0]
    width = out_ref.shape[0]
    back = back_ref[...].astype(F32).T.astype(BF16)
    total = jnp.zeros(out_ref.shape, F32)
    for h in range(2):
        piece = back[h * width : (h + 1) * width]
        for part in (first_ref, rest_ref):
            total = total + dot(piece, part[h * count : (h + 1) * count])
    out_ref[...] = total.astype(BF16)


def call(kernel, out_shapes, *args, flops=1 << 24, scratch=()):
    single = not isinstance(out_shapes, list)
    specs = [pl.BlockSpec(memory_space=pltpu.VMEM)] * len(args)
    outs = [out_shapes] if single else out_shapes
    out_specs = [pl.BlockSpec(memory_space=pltpu.VMEM)] * len(outs)
    return pl.pallas_call(
        kernel,
        out_shape=out_shapes,
        in_specs=specs,
        out_specs=out_specs[0] if single else out_specs,
        scratch_shapes=list(scratch),
        cost_estimate=pl.CostEstimate(flops=flops, bytes_accessed=1 << 20, transcendentals=0),
        compiler_params=pltpu.CompilerParams(vmem_limit_bytes=16 << 20),
    )(*args)


def gathered(shard, axis):
    count = lax.axis_size(axis)
    me = lax.axis_index(axis)
    whole = jnp.zeros((count,) + shard.shape, shard.dtype)
    whole = lax.dynamic_update_slice_in_dim(whole, shard[None], me, 0)
    for hop in range(1, count):
        piece = lax.ppermute(shard, axis, [(i, (i + hop) % count) for i in range(count)])
        source = lax.rem(me + (count - hop), count)
        whole = lax.dynamic_update_slice_in_dim(whole, piece[None], source, 0)
    return whole


def body(tokens, norm_gain, gate_weight, up_weight, down_weight, expert_ids, route_weight):
    tok_rows, top = expert_ids.shape
    width = tokens.shape[1]
    full = norm_gain.shape[0]
    ep, ny, nx = lax.axis_size(EP), lax.axis_size(TY), lax.axis_size(TX)
    tp = ny * nx
    units = gate_weight.shape[2]
    half = tok_rows * top // ep
    count, wide = ep * half, 2 * width
    group = count // nx
    shape = jax.ShapeDtypeStruct

    sent, place = call(
        functools.partial(prep_kernel, ep),
        [shape((count, wide), BF16), shape((top, tok_rows), I32)],
        expert_ids.T,
        tokens.T,
    )
    got = lax.all_to_all(sent.reshape(ep, half, wide), EP, 0, 0, tiled=True)

    shard = jnp.stack([w[0].T for w in (gate_weight, up_weight, down_weight)])
    weights = gathered(shard, TX)

    spread = call(spread_kernel, shape((ny, nx, group, wide), BF16), got.reshape(count, wide))
    rows = lax.all_to_all(spread.reshape(tp, group, wide), TP, 0, 0, tiled=True)
    hidden = call(
        up_kernel,
        shape((ny, 2 * group, nx * units), BF16),
        rows,
        norm_gain.astype(F32).reshape(1, full),
        weights,
        flops=1 << 28,
        scratch=(pltpu.VMEM((2 * group, full), F32), pltpu.VMEM((2 * group, full), BF16)),
    )
    hidden = lax.all_to_all(hidden, TY, 0, 0, tiled=True)
    out = call(down_kernel, shape((count, wide), BF16), hidden, weights, flops=1 << 27)

    back = lax.all_to_all(out.reshape(ep * nx, half // nx, wide), (EP, TX), 0, 0, tiled=True)
    first, rest = call(
        mix_kernel,
        [shape((2 * count, tok_rows), BF16)] * 2,
        place,
        route_weight.astype(F32).T,
    )
    combined = call(
        combine_kernel, shape((width, tok_rows), BF16), back.reshape(count, wide), first, rest
    )
    return combined.T


def solution(mesh):
    devices = mesh.devices.reshape(mesh.shape["ep"], 4, 4)
    split = Mesh(devices, (EP, TY, TX))
    in_specs = (
        P(EP, TP),
        P(),
        P(EP, None, TP),
        P(EP, None, TP),
        P(EP, None, TP),
        P(EP, None),
        P(EP, None),
    )
    return jax.shard_map(body, mesh=split, in_specs=in_specs, out_specs=P(EP, TP), check_vma=False)
```

```python
import functools

import jax
import jax.numpy as jnp
from jax import lax
from jax.experimental import pallas as pl
from jax.experimental.pallas import tpu as pltpu
from jax.sharding import Mesh
from jax.sharding import PartitionSpec as P


Z, CORE, TY, TX = "z", "core", "ty", "tx"
EP, TP = (Z, CORE), (TY, TX)
EPSILON = 1e-06
ALPHA = 1.702
LIMIT = 7.0
BF16, F32, I32 = jnp.bfloat16, jnp.float32, jnp.int32
NT = (((1,), (1,)), ((), ()))


def iota(shape, dim):
    return lax.broadcasted_iota(I32, shape, dim)


def dot(a, b):
    return jnp.dot(a, b, preferred_element_type=F32)


def dot_nt(a, b):
    return lax.dot_general(a, b, NT, preferred_element_type=F32)


def ones_where(mask):
    return jnp.where(mask, 1.0, 0.0).astype(BF16)


def moved(rows, sizes, order):
    count = rows.shape[0]
    left, source = iota((count, 1), 0), jnp.zeros((count, 1), I32)
    for axis in reversed(order):
        stride = 1
        for size in sizes[axis + 1 :]:
            stride *= size
        source = source + (left & (sizes[axis] - 1)) * stride
        left = left >> (sizes[axis].bit_length() - 1)
    select = ones_where(iota((count, count), 1) == source)
    return dot(select, rows).astype(BF16)


def halves(first, second):
    wide = first.shape[1] // 2
    left = iota(first.shape, 1) < wide
    return (
        jnp.where(left, first, pltpu.roll(second, wide, 1)),
        jnp.where(left, pltpu.roll(first, wide, 1), second),
    )


def prep_kernel(
    sizes, ids_hbm, tokens_hbm, gate_hbm, up_hbm, down_hbm, sent_ref, place_ref, shard_ref,
    ids_ref, tokens_ref, sems
):
    nz, cores, nx = sizes
    small = [(ids_hbm, ids_ref), (tokens_hbm, tokens_ref)]
    large = [(w, shard_ref.at[i]) for i, w in enumerate((gate_hbm, up_hbm, down_hbm))]
    copies = [pltpu.make_async_copy(a, b, sems.at[i]) for i, (a, b) in enumerate(small + large)]
    for copy in copies:
        copy.start()
    top, toks = ids_ref.shape
    count, _ = sent_ref.shape
    experts = nz * cores
    half = count // experts
    inner = half // nx
    earlier = ones_where(iota((toks, toks), 0) < iota((toks, toks), 1))
    expert = iota((experts, toks), 0)
    copies[0].wait()
    ids = ids_ref[...]
    picks = [expert == ids[k : k + 1] for k in range(top)]
    named = picks[0]
    for pick in picks[1:]:
        named = named | pick
    before = dot(ones_where(named), earlier)
    lane = iota((2 * count, toks), 0)
    hit = None
    for k in range(top):
        slot = jnp.sum(jnp.where(picks[k], before, 0.0), axis=0, keepdims=True).astype(I32)
        low, high = slot & (half - 1), jnp.where(slot >= half, count, 0)
        owner = ids[k : k + 1]
        place_ref[k : k + 1] = owner * half + low + high
        x, r = low >> (inner.bit_length() - 1), low & (inner - 1)
        z, core = owner >> (cores.bit_length() - 1), owner & (cores - 1)
        place = ((z * nx + x) * cores + core) * inner + r + high
        hit = (lane == place) if hit is None else hit | (lane == place)
    select = ones_where(hit)
    copies[1].wait()
    tokens = tokens_ref[...].astype(F32)
    zero = jnp.zeros_like(tokens)
    both = jnp.concatenate(
        [jnp.concatenate([tokens, zero], 1), jnp.concatenate([zero, tokens], 1)], 0
    ).astype(BF16)
    both_select = jnp.concatenate([select[:count], select[count:]], 1)
    sent_ref[...] = dot_nt(both_select, both).astype(BF16)
    for copy in copies[2:]:
        copy.wait()


def mix_kernel(place_ref, weight_ref, first_ref, rest_ref):
    count, toks = first_ref.shape
    lane = iota((count, toks), 0)
    mix = jnp.zeros((count, toks), F32)
    for k in range(place_ref.shape[0]):
        mix = mix + jnp.where(lane == place_ref[k : k + 1], weight_ref[k : k + 1], 0.0)
    first = mix.astype(BF16)
    first_ref[...] = first
    rest_ref[...] = (mix - first.astype(F32)).astype(BF16)


def spread_kernel(sizes, got_ref, out_ref):
    cores, copies, _, _, _ = out_ref.shape
    rows = moved(got_ref[...], sizes, (2, 1, 0, 3)).reshape((cores,) + out_ref.shape[2:])
    for core in range(cores):
        for c in range(copies):
            out_ref[core, c] = rows[core]


def up_kernel(rows_ref, gain_ref, weights_ref, out_ref, whole, normed):
    cores, pieces, part, wide = rows_ref.shape
    group = cores * part
    full = normed.shape[1]
    squares = [jnp.zeros((group, wide), F32) for _ in range(2)]
    for j in range(pieces // 2):
        even, odd = (
            jnp.concatenate([rows_ref[c, 2 * j + i].astype(F32) for c in range(cores)], 0)
            for i in range(2)
        )
        pair = halves(even, odd)
        for h in range(2):
            whole[h * group : (h + 1) * group, j * wide : (j + 1) * wide] = pair[h]
            squares[h] = squares[h] + pair[h] * pair[h]
    for h in range(2):
        mean = jnp.sum(squares[h], axis=1, keepdims=True) / full
        inverse = lax.rsqrt(mean + EPSILON)
        rows = slice(h * group, (h + 1) * group)
        normed[rows] = (whole[rows] * inverse * gain_ref[...]).astype(BF16)
    nx, _, units, _ = weights_ref.shape
    w_gate = weights_ref[:, 0].reshape(nx * units, full)
    w_up = weights_ref[:, 1].reshape(nx * units, full)
    gate = jnp.minimum(dot_nt(normed[...], w_gate), LIMIT)
    up = jnp.clip(dot_nt(normed[...], w_up), -LIMIT, LIMIT)
    hidden = ((up + 1.0) * gate * jax.nn.sigmoid(ALPHA * gate)).astype(BF16)
    for c in range(out_ref.shape[0]):
        out_ref[c] = hidden


def down_kernel(sizes, hidden_ref, weights_ref, out_ref):
    ny, rows, units = hidden_ref.shape
    nx, _, width, full = weights_ref.shape
    w_down = weights_ref[:, 2].reshape(nx * width, full)
    total = dot_nt(hidden_ref[0], w_down[:, :units])
    for y in range(1, ny):
        total = total + dot_nt(hidden_ref[y], w_down[:, y * units : (y + 1) * units])
    group = rows // 2
    pieces = []
    for j in range(nx // 2):
        lanes = slice(2 * j * width, 2 * (j + 1) * width)
        pieces += halves(total[:group, lanes], total[group:, lanes])
    stacked = jnp.concatenate(pieces, 0).astype(BF16)
    out_ref[...] = moved(stacked, sizes, (2, 1, 0, 3))


def combine_kernel(back_ref, first_ref, rest_ref, out_ref):
    count = back_ref.shape[0]
    width = out_ref.shape[0]
    back = back_ref[...].astype(F32).T.astype(BF16)
    total = jnp.zeros(out_ref.shape, F32)
    for h in range(2):
        piece = back[h * width : (h + 1) * width]
        for part in (first_ref, rest_ref):
            total = total + dot(piece, part[h * count : (h + 1) * count])
    out_ref[...] = total.astype(BF16)


def call(kernel, out_shapes, *args, flops=1 << 24, scratch=(), space=pltpu.VMEM, vmem=16):
    single = not isinstance(out_shapes, list)
    outs = [out_shapes] if single else out_shapes
    out_specs = [pl.BlockSpec(memory_space=pltpu.VMEM)] * len(outs)
    return pl.pallas_call(
        kernel,
        out_shape=out_shapes,
        in_specs=[pl.BlockSpec(memory_space=space)] * len(args),
        out_specs=out_specs[0] if single else out_specs,
        scratch_shapes=list(scratch),
        cost_estimate=pl.CostEstimate(flops=flops, bytes_accessed=1 << 20, transcendentals=0),
        compiler_params=pltpu.CompilerParams(vmem_limit_bytes=vmem << 20),
    )(*args)


def gathered(shard, axis):
    count = lax.axis_size(axis)
    me = lax.axis_index(axis)
    whole = jnp.zeros((count,) + shard.shape, shard.dtype)
    whole = lax.dynamic_update_slice_in_dim(whole, shard[None], me, 0)
    for hop in range(1, count):
        piece = lax.ppermute(shard, axis, [(i, (i + hop) % count) for i in range(count)])
        source = lax.rem(me + (count - hop), count)
        whole = lax.dynamic_update_slice_in_dim(whole, piece[None], source, 0)
    return whole


def body(tokens, norm_gain, gate_weight, up_weight, down_weight, expert_ids, route_weight):
    tok_rows, top = expert_ids.shape
    width = tokens.shape[1]
    full = norm_gain.shape[0]
    nz, cores, ny, nx = (lax.axis_size(axis) for axis in (Z, CORE, TY, TX))
    ep, tp = nz * cores, ny * nx
    units = gate_weight.shape[2]
    half = tok_rows * top // ep
    inner = half // nx
    count, wide = ep * half, 2 * width
    group = count // nx
    shape = jax.ShapeDtypeStruct

    sent, place, shard = call(
        functools.partial(prep_kernel, (nz, cores, nx)),
        [
            shape((count, wide), BF16),
            shape((top, tok_rows), I32),
            shape((3, units, full), BF16),
        ],
        expert_ids.T,
        tokens.T,
        gate_weight[0].T,
        up_weight[0].T,
        down_weight[0].T,
        scratch=(
            pltpu.VMEM((top, tok_rows), I32),
            pltpu.VMEM((width, tok_rows), BF16),
            pltpu.SemaphoreType.DMA((5,)),
        ),
        space=pltpu.HBM,
        vmem=62,
    )
    got = lax.all_to_all(
        sent.reshape(nz * nx, cores * inner, wide), (Z, TX), 0, 0, tiled=True
    )
    weights = gathered(shard, TX)

    spread = call(
        functools.partial(spread_kernel, (nz, nx, cores, inner)),
        shape((cores, ny, nx, nz * inner, wide), BF16),
        got.reshape(count, wide),
    )
    rows = lax.all_to_all(
        spread.reshape(cores * ny, nx * nz * inner, wide), (CORE, TY), 0, 0, tiled=True
    )
    hidden = call(
        up_kernel,
        shape((ny, 2 * group, nx * units), BF16),
        rows.reshape(cores, tp, nz * inner, wide),
        norm_gain.astype(F32).reshape(1, full),
        weights,
        flops=1 << 28,
        scratch=(pltpu.VMEM((2 * group, full), F32), pltpu.VMEM((2 * group, full), BF16)),
    )
    hidden = lax.all_to_all(hidden, TY, 0, 0, tiled=True)
    out = call(
        functools.partial(down_kernel, (nx, cores, nz, inner)),
        shape((count, wide), BF16),
        hidden,
        weights,
        flops=1 << 27,
    )

    back = lax.all_to_all(
        out.reshape(ep * nx, inner, wide), (Z, CORE, TX), 0, 0, tiled=True
    )
    first, rest = call(
        mix_kernel,
        [shape((2 * count, tok_rows), BF16)] * 2,
        place,
        route_weight.astype(F32).T,
    )
    combined = call(
        combine_kernel, shape((width, tok_rows), BF16), back.reshape(count, wide), first, rest
    )
    return combined.T


def solution(mesh):
    devices = mesh.devices.reshape(mesh.shape["ep"] // 2, 2, 4, 4)
    split = Mesh(devices, (Z, CORE, TY, TX))
    in_specs = (
        P(EP, TP),
        P(),
        P(EP, None, TP),
        P(EP, None, TP),
        P(EP, None, TP),
        P(EP, None),
        P(EP, None),
    )
    return jax.shard_map(body, mesh=split, in_specs=in_specs, out_specs=P(EP, TP), check_vma=False)
```

```python
import functools

import jax
import jax.numpy as jnp
from jax import lax
from jax.experimental import pallas as pl
from jax.experimental.pallas import tpu as pltpu
from jax.sharding import Mesh
from jax.sharding import PartitionSpec as P


Z, CORE, TY, TX = "z", "core", "ty", "tx"
EP, TP = (Z, CORE), (TY, TX)
EPSILON = 1e-06
ALPHA = 1.702
LIMIT = 7.0
BF16, F32, I32 = jnp.bfloat16, jnp.float32, jnp.int32
NT = (((1,), (1,)), ((), ()))


def iota(shape, dim):
    return lax.broadcasted_iota(I32, shape, dim)


def dot(a, b):
    return jnp.dot(a, b, preferred_element_type=F32)


def dot_nt(a, b):
    return lax.dot_general(a, b, NT, preferred_element_type=F32)


def ones_where(mask):
    return jnp.where(mask, 1.0, 0.0).astype(BF16)


def quads(first, second):
    half = first.shape[1] // 2
    top = iota(first.shape, 1) < half
    return (
        jnp.where(top, first, pltpu.roll(second, half, 1)),
        jnp.where(top, pltpu.roll(first, half, 1), second),
    )


def halves(first, second):
    wide = first.shape[1] // 2
    left = iota(first.shape, 1) < wide
    return (
        jnp.where(left, first, pltpu.roll(second, wide, 1)),
        jnp.where(left, pltpu.roll(first, wide, 1), second),
    )


def prep_kernel(
    sizes, ids_hbm, tokens_hbm, gate_hbm, up_hbm, down_hbm, sent_ref, place_ref, shard_ref,
    ids_ref, tokens_ref, sems
):
    nz, cores, nx = sizes
    small = [(ids_hbm, ids_ref), (tokens_hbm, tokens_ref)]
    large = [(w, shard_ref.at[i]) for i, w in enumerate((gate_hbm, up_hbm, down_hbm))]
    copies = [pltpu.make_async_copy(a, b, sems.at[i]) for i, (a, b) in enumerate(small + large)]
    for copy in copies:
        copy.start()
    top, toks = ids_ref.shape
    count, _ = sent_ref.shape
    experts = nz * cores
    half = count // experts
    inner = half // nx
    earlier = ones_where(iota((toks, toks), 0) < iota((toks, toks), 1))
    expert = iota((experts, toks), 0)
    copies[0].wait()
    ids = ids_ref[...]
    picks = [expert == ids[k : k + 1] for k in range(top)]
    named = picks[0]
    for pick in picks[1:]:
        named = named | pick
    before = dot(ones_where(named), earlier)
    lane = iota((2 * count, toks), 0)
    hit = None
    for k in range(top):
        slot = jnp.sum(jnp.where(picks[k], before, 0.0), axis=0, keepdims=True).astype(I32)
        low, high = slot & (half - 1), jnp.where(slot >= half, count, 0)
        owner = ids[k : k + 1]
        place_ref[k : k + 1] = owner * half + low + high
        x, r = low >> (inner.bit_length() - 1), low & (inner - 1)
        z, core = owner >> (cores.bit_length() - 1), owner & (cores - 1)
        place = ((z * nx + x) * cores + core) * inner + r + high
        hit = (lane == place) if hit is None else hit | (lane == place)
    select = ones_where(hit)
    copies[1].wait()
    tokens = tokens_ref[...].astype(F32)
    zero = jnp.zeros_like(tokens)
    both = jnp.concatenate(
        [jnp.concatenate([tokens, zero], 1), jnp.concatenate([zero, tokens], 1)], 0
    ).astype(BF16)
    both_select = jnp.concatenate([select[:count], select[count:]], 1)
    sent_ref[...] = dot_nt(both_select, both).astype(BF16)
    for copy in copies[2:]:
        copy.wait()


def mix_kernel(place_ref, weight_ref, first_ref, rest_ref):
    count, toks = first_ref.shape
    lane = iota((count, toks), 0)
    mix = jnp.zeros((count, toks), F32)
    for k in range(place_ref.shape[0]):
        mix = mix + jnp.where(lane == place_ref[k : k + 1], weight_ref[k : k + 1], 0.0)
    first = mix.astype(BF16)
    first_ref[...] = first
    rest_ref[...] = (mix - first.astype(F32)).astype(BF16)


def spread_kernel(got_ref, out_ref, turned):
    cores, copies, nx, rows, wide = out_ref.shape
    got = got_ref[...].astype(F32).reshape(-1, 2, nx, 8, wide)
    for x in range(nx):
        for core, part in enumerate(quads(got[:, 0, x], got[:, 1, x])):
            turned[core, x] = part.reshape(rows, wide)
    for core in range(cores):
        for x in range(nx):
            part = turned[core, x].astype(BF16)
            for c in range(copies):
                out_ref[core, c, x] = part


def up_kernel(rows_ref, gain_ref, weights_ref, out_ref, whole, normed):
    cores, pieces, part, wide = rows_ref.shape
    group = cores * part
    full = normed.shape[1]
    squares = [jnp.zeros((group, wide), F32) for _ in range(2)]
    for j in range(pieces // 2):
        even, odd = (
            jnp.concatenate([rows_ref[c, 2 * j + i].astype(F32) for c in range(cores)], 0)
            for i in range(2)
        )
        pair = halves(even, odd)
        for h in range(2):
            whole[h * group : (h + 1) * group, j * wide : (j + 1) * wide] = pair[h]
            squares[h] = squares[h] + pair[h] * pair[h]
    for h in range(2):
        mean = jnp.sum(squares[h], axis=1, keepdims=True) / full
        inverse = lax.rsqrt(mean + EPSILON)
        rows = slice(h * group, (h + 1) * group)
        normed[rows] = (whole[rows] * inverse * gain_ref[...]).astype(BF16)
    nx, _, units, _ = weights_ref.shape
    w_gate = weights_ref[:, 0].reshape(nx * units, full)
    w_up = weights_ref[:, 1].reshape(nx * units, full)
    gate = jnp.minimum(dot_nt(normed[...], w_gate), LIMIT)
    up = jnp.clip(dot_nt(normed[...], w_up), -LIMIT, LIMIT)
    hidden = ((up + 1.0) * gate * jax.nn.sigmoid(ALPHA * gate)).astype(BF16)
    for c in range(out_ref.shape[0]):
        out_ref[c] = hidden


def down_kernel(cores, hidden_ref, weights_ref, out_ref, turned):
    ny, rows, units = hidden_ref.shape
    nx, _, width, full = weights_ref.shape
    w_down = weights_ref[:, 2].reshape(nx * width, full)
    total = dot_nt(hidden_ref[0], w_down[:, :units])
    for y in range(1, ny):
        total = total + dot_nt(hidden_ref[y], w_down[:, y * units : (y + 1) * units])
    group = rows // 2
    pieces = []
    for j in range(nx // 2):
        lanes = slice(2 * j * width, 2 * (j + 1) * width)
        pieces += halves(total[:group, lanes], total[group:, lanes])
    for j in range(nx // 2):
        first, second = (p.reshape(-1, 8, 2 * width) for p in pieces[2 * j : 2 * j + 2])
        for odd, part in enumerate(quads(first, second)):
            part = part.reshape(cores, -1, 8, 2 * width)
            for core in range(cores):
                turned[:, odd, core, j] = part[core]
    out_ref[...] = turned[...].reshape(out_ref.shape).astype(BF16)


def combine_kernel(back_ref, first_ref, rest_ref, out_ref):
    count = back_ref.shape[0]
    width = out_ref.shape[0]
    back = back_ref[...].astype(F32).T.astype(BF16)
    total = jnp.zeros(out_ref.shape, F32)
    for h in range(2):
        piece = back[h * width : (h + 1) * width]
        for part in (first_ref, rest_ref):
            total = total + dot(piece, part[h * count : (h + 1) * count])
    out_ref[...] = total.astype(BF16)


def call(kernel, out_shapes, *args, flops=1 << 24, scratch=(), space=pltpu.VMEM, vmem=16):
    single = not isinstance(out_shapes, list)
    outs = [out_shapes] if single else out_shapes
    out_specs = [pl.BlockSpec(memory_space=pltpu.VMEM)] * len(outs)
    return pl.pallas_call(
        kernel,
        out_shape=out_shapes,
        in_specs=[pl.BlockSpec(memory_space=space)] * len(args),
        out_specs=out_specs[0] if single else out_specs,
        scratch_shapes=list(scratch),
        cost_estimate=pl.CostEstimate(flops=flops, bytes_accessed=1 << 20, transcendentals=0),
        compiler_params=pltpu.CompilerParams(vmem_limit_bytes=vmem << 20),
    )(*args)


def gathered(shard, axis):
    count = lax.axis_size(axis)
    me = lax.axis_index(axis)
    whole = jnp.zeros((count,) + shard.shape, shard.dtype)
    whole = lax.dynamic_update_slice_in_dim(whole, shard[None], me, 0)
    for hop in range(1, count):
        piece = lax.ppermute(shard, axis, [(i, (i + hop) % count) for i in range(count)])
        source = lax.rem(me + (count - hop), count)
        whole = lax.dynamic_update_slice_in_dim(whole, piece[None], source, 0)
    return whole


def body(tokens, norm_gain, gate_weight, up_weight, down_weight, expert_ids, route_weight):
    tok_rows, top = expert_ids.shape
    width = tokens.shape[1]
    full = norm_gain.shape[0]
    nz, cores, ny, nx = (lax.axis_size(axis) for axis in (Z, CORE, TY, TX))
    ep, tp = nz * cores, ny * nx
    units = gate_weight.shape[2]
    half = tok_rows * top // ep
    inner = half // nx
    count, wide = ep * half, 2 * width
    group = count // nx
    shape = jax.ShapeDtypeStruct

    sent, place, shard = call(
        functools.partial(prep_kernel, (nz, cores, nx)),
        [
            shape((count, wide), BF16),
            shape((top, tok_rows), I32),
            shape((3, units, full), BF16),
        ],
        expert_ids.T,
        tokens.T,
        gate_weight[0].T,
        up_weight[0].T,
        down_weight[0].T,
        scratch=(
            pltpu.VMEM((top, tok_rows), I32),
            pltpu.VMEM((width, tok_rows), BF16),
            pltpu.SemaphoreType.DMA((5,)),
        ),
        space=pltpu.HBM,
        vmem=62,
    )
    got = lax.all_to_all(
        sent.reshape(nz * nx, cores * inner, wide), (Z, TX), 0, 0, tiled=True
    )
    weights = gathered(shard, TX)

    spread = call(
        spread_kernel,
        shape((cores, ny, nx, nz * inner, wide), BF16),
        got.reshape(count, wide),
        scratch=(pltpu.VMEM((cores, nx, nz * inner, wide), F32),),
    )
    rows = lax.all_to_all(
        spread.reshape(cores * ny, nx * nz * inner, wide), (CORE, TY), 0, 0, tiled=True
    )
    hidden = call(
        up_kernel,
        shape((ny, 2 * group, nx * units), BF16),
        rows.reshape(cores, tp, nz * inner, wide),
        norm_gain.astype(F32).reshape(1, full),
        weights,
        flops=1 << 28,
        scratch=(pltpu.VMEM((2 * group, full), F32), pltpu.VMEM((2 * group, full), BF16)),
    )
    hidden = lax.all_to_all(hidden, TY, 0, 0, tiled=True)
    out = call(
        functools.partial(down_kernel, cores),
        shape((count, wide), BF16),
        hidden,
        weights,
        flops=1 << 27,
        scratch=(pltpu.VMEM((nz // 2, 2, cores, nx // 2, 2 * inner, wide), F32),),
    )

    back = lax.all_to_all(
        out.reshape(ep * nx, inner, wide), (Z, CORE, TX), 0, 0, tiled=True
    )
    first, rest = call(
        mix_kernel,
        [shape((2 * count, tok_rows), BF16)] * 2,
        place,
        route_weight.astype(F32).T,
    )
    combined = call(
        combine_kernel, shape((width, tok_rows), BF16), back.reshape(count, wide), first, rest
    )
    return combined.T


def solution(mesh):
    devices = mesh.devices.reshape(mesh.shape["ep"] // 2, 2, 4, 4)
    split = Mesh(devices, (Z, CORE, TY, TX))
    in_specs = (
        P(EP, TP),
        P(),
        P(EP, None, TP),
        P(EP, None, TP),
        P(EP, None, TP),
        P(EP, None),
        P(EP, None),
    )
    return jax.shard_map(body, mesh=split, in_specs=in_specs, out_specs=P(EP, TP), check_vma=False)
```

```python
import functools

import jax
import jax.numpy as jnp
from jax import lax
from jax.experimental import pallas as pl
from jax.experimental.pallas import tpu as pltpu
from jax.sharding import Mesh
from jax.sharding import PartitionSpec as P


Z, CORE, TY, TX = "z", "core", "ty", "tx"
EP, TP = (Z, CORE), (TY, TX)
EPSILON = 1e-06
ALPHA = 1.702
LIMIT = 7.0
BF16, F32, I32 = jnp.bfloat16, jnp.float32, jnp.int32
NT = (((1,), (1,)), ((), ()))


def iota(shape, dim):
    return lax.broadcasted_iota(I32, shape, dim)


def dot(a, b):
    return jnp.dot(a, b, preferred_element_type=F32)


def dot_nt(a, b):
    return lax.dot_general(a, b, NT, preferred_element_type=F32)


def ones_where(mask):
    return jnp.where(mask, 1.0, 0.0).astype(BF16)


def quads(first, second):
    half = first.shape[1] // 2
    top = iota(first.shape, 1) < half
    return (
        jnp.where(top, first, pltpu.roll(second, half, 1)),
        jnp.where(top, pltpu.roll(first, half, 1), second),
    )


def halves(first, second):
    wide = first.shape[1] // 2
    left = iota(first.shape, 1) < wide
    return (
        jnp.where(left, first, pltpu.roll(second, wide, 1)),
        jnp.where(left, pltpu.roll(first, wide, 1), second),
    )


def prep_kernel(
    sizes, ids_hbm, tokens_hbm, gate_hbm, up_hbm, down_hbm, sent_ref, place_ref, shard_ref,
    ids_ref, tokens_ref, sems
):
    nz, cores, nx = sizes
    small = [(ids_hbm, ids_ref), (tokens_hbm, tokens_ref)]
    large = [(w, shard_ref.at[i]) for i, w in enumerate((gate_hbm, up_hbm, down_hbm))]
    copies = [pltpu.make_async_copy(a, b, sems.at[i]) for i, (a, b) in enumerate(small + large)]
    for copy in copies:
        copy.start()
    top, toks = ids_ref.shape
    count, _ = sent_ref.shape
    experts = nz * cores
    half = count // experts
    inner = half // nx
    earlier = ones_where(iota((toks, toks), 0) < iota((toks, toks), 1))
    expert = iota((experts, toks), 0)
    copies[0].wait()
    ids = ids_ref[...]
    picks = [expert == ids[k : k + 1] for k in range(top)]
    named = picks[0]
    for pick in picks[1:]:
        named = named | pick
    before = dot(ones_where(named), earlier)
    lane = iota((2 * count, toks), 0)
    hit = None
    for k in range(top):
        slot = jnp.sum(jnp.where(picks[k], before, 0.0), axis=0, keepdims=True).astype(I32)
        low, high = slot & (half - 1), jnp.where(slot >= half, count, 0)
        owner = ids[k : k + 1]
        place_ref[k : k + 1] = owner * half + low + high
        x, r = low >> (inner.bit_length() - 1), low & (inner - 1)
        z, core = owner >> (cores.bit_length() - 1), owner & (cores - 1)
        place = ((z * nx + x) * cores + core) * inner + r + high
        hit = (lane == place) if hit is None else hit | (lane == place)
    select = ones_where(hit)
    copies[1].wait()
    tokens = tokens_ref[...].astype(F32)
    zero = jnp.zeros_like(tokens)
    both = jnp.concatenate(
        [jnp.concatenate([tokens, zero], 1), jnp.concatenate([zero, tokens], 1)], 0
    ).astype(BF16)
    both_select = jnp.concatenate([select[:count], select[count:]], 1)
    sent_ref[...] = dot_nt(both_select, both).astype(BF16)
    for copy in copies[2:]:
        copy.wait()


def mix_kernel(place_ref, weight_ref, first_ref, rest_ref):
    count, toks = first_ref.shape
    lane = iota((count, toks), 0)
    mix = jnp.zeros((count, toks), F32)
    for k in range(place_ref.shape[0]):
        mix = mix + jnp.where(lane == place_ref[k : k + 1], weight_ref[k : k + 1], 0.0)
    first = mix.astype(BF16)
    first_ref[...] = first
    rest_ref[...] = (mix - first.astype(F32)).astype(BF16)


def spread_kernel(got_ref, out_ref, turned):
    cores, copies, nx, rows, wide = out_ref.shape
    got = got_ref[...].astype(F32).reshape(-1, 2, nx, 8, wide)
    for x in range(nx):
        for core, part in enumerate(quads(got[:, 0, x], got[:, 1, x])):
            turned[core, x] = part.reshape(rows, wide)
    for core in range(cores):
        for x in range(nx):
            part = turned[core, x].astype(BF16)
            for c in range(copies):
                out_ref[core, c, x] = part


def up_kernel(rows_ref, gain_ref, weights_ref, out_ref, whole, normed):
    cores, pieces, part, wide = rows_ref.shape
    group = cores * part
    full = normed.shape[1]
    squares = [jnp.zeros((group, wide), F32) for _ in range(2)]
    for j in range(pieces // 2):
        even, odd = (
            jnp.concatenate([rows_ref[c, 2 * j + i].astype(F32) for c in range(cores)], 0)
            for i in range(2)
        )
        pair = halves(even, odd)
        for h in range(2):
            whole[h * group : (h + 1) * group, j * wide : (j + 1) * wide] = pair[h]
            squares[h] = squares[h] + pair[h] * pair[h]
    for h in range(2):
        mean = jnp.sum(squares[h], axis=1, keepdims=True) / full
        inverse = lax.rsqrt(mean + EPSILON)
        rows = slice(h * group, (h + 1) * group)
        normed[rows] = (whole[rows] * inverse * gain_ref[...]).astype(BF16)
    nx, _, units, _ = weights_ref.shape
    w_gate = weights_ref[:, 0].reshape(nx * units, full)
    w_up = weights_ref[:, 1].reshape(nx * units, full)
    gate = jnp.minimum(dot_nt(normed[...], w_gate), LIMIT)
    up = jnp.clip(dot_nt(normed[...], w_up), -LIMIT, LIMIT)
    hidden = ((up + 1.0) * gate * jax.nn.sigmoid(ALPHA * gate)).astype(BF16)
    for c in range(out_ref.shape[0]):
        out_ref[c] = hidden


def down_kernel(cores, hidden_ref, weights_ref, out_ref, turned):
    ny, rows, units = hidden_ref.shape
    nx, width, full = weights_ref.shape
    w_down = weights_ref[...].reshape(nx * width, full)
    total = dot_nt(hidden_ref[0], w_down[:, :units])
    for y in range(1, ny):
        total = total + dot_nt(hidden_ref[y], w_down[:, y * units : (y + 1) * units])
    group = rows // 2
    pieces = []
    for j in range(nx // 2):
        lanes = slice(2 * j * width, 2 * (j + 1) * width)
        pieces += halves(total[:group, lanes], total[group:, lanes])
    for j in range(nx // 2):
        first, second = (p.reshape(-1, 8, 2 * width) for p in pieces[2 * j : 2 * j + 2])
        for odd, part in enumerate(quads(first, second)):
            part = part.reshape(cores, -1, 8, 2 * width)
            for core in range(cores):
                turned[:, odd, core, j] = part[core]
    out_ref[...] = turned[...].reshape(out_ref.shape).astype(BF16)


def combine_kernel(back_ref, first_ref, rest_ref, out_ref):
    count = back_ref.shape[0]
    width = out_ref.shape[0]
    back = back_ref[...].astype(F32).T.astype(BF16)
    total = jnp.zeros(out_ref.shape, F32)
    for h in range(2):
        piece = back[h * width : (h + 1) * width]
        for part in (first_ref, rest_ref):
            total = total + dot(piece, part[h * count : (h + 1) * count])
    out_ref[...] = total.astype(BF16)


def call(kernel, out_shapes, *args, flops=1 << 24, scratch=(), space=pltpu.VMEM, vmem=16):
    single = not isinstance(out_shapes, list)
    outs = [out_shapes] if single else out_shapes
    out_specs = [pl.BlockSpec(memory_space=pltpu.VMEM)] * len(outs)
    return pl.pallas_call(
        kernel,
        out_shape=out_shapes,
        in_specs=[pl.BlockSpec(memory_space=space)] * len(args),
        out_specs=out_specs[0] if single else out_specs,
        scratch_shapes=list(scratch),
        cost_estimate=pl.CostEstimate(flops=flops, bytes_accessed=1 << 20, transcendentals=0),
        compiler_params=pltpu.CompilerParams(vmem_limit_bytes=vmem << 20),
    )(*args)


def set_at(whole, piece, index):
    return lax.dynamic_update_slice_in_dim(whole, piece[None], index, 0)


def gathered(shard):
    count = lax.axis_size(TX)
    me = lax.axis_index(TX)
    near, after = ([(i, (i + hop) % count) for i in range(count)] for hop in (1, count - 1))
    left = lax.ppermute(shard, TX, near)
    right = lax.ppermute(shard, TX, after)
    far_up = lax.ppermute(left[:2], TX, near)
    far_down = lax.ppermute(right[2], TX, after)
    up = jnp.zeros((count, 2) + shard.shape[1:], shard.dtype)
    down = jnp.zeros((count,) + shard.shape[1:], shard.dtype)
    up, down = set_at(up, shard[:2], me), set_at(down, shard[2], me)
    before, behind, across = (lax.rem(me + hop, count) for hop in (count - 1, 1, count - 2))
    for piece, source in ((left, before), (right, behind)):
        up = set_at(up, piece[:2], source)
    up = set_at(up, far_up, across)
    for piece, source in ((left, before), (right, behind)):
        down = set_at(down, piece[2], source)
    down = set_at(down, far_down, across)
    return up, down


def body(tokens, norm_gain, gate_weight, up_weight, down_weight, expert_ids, route_weight):
    tok_rows, top = expert_ids.shape
    width = tokens.shape[1]
    full = norm_gain.shape[0]
    nz, cores, ny, nx = (lax.axis_size(axis) for axis in (Z, CORE, TY, TX))
    ep, tp = nz * cores, ny * nx
    units = gate_weight.shape[2]
    half = tok_rows * top // ep
    inner = half // nx
    count, wide = ep * half, 2 * width
    group = count // nx
    shape = jax.ShapeDtypeStruct

    sent, place, shard = call(
        functools.partial(prep_kernel, (nz, cores, nx)),
        [
            shape((count, wide), BF16),
            shape((top, tok_rows), I32),
            shape((3, units, full), BF16),
        ],
        expert_ids.T,
        tokens.T,
        gate_weight[0].T,
        up_weight[0].T,
        down_weight[0].T,
        scratch=(
            pltpu.VMEM((top, tok_rows), I32),
            pltpu.VMEM((width, tok_rows), BF16),
            pltpu.SemaphoreType.DMA((5,)),
        ),
        space=pltpu.HBM,
        vmem=62,
    )
    got = lax.all_to_all(
        sent.reshape(nz * nx, cores * inner, wide), (Z, TX), 0, 0, tiled=True
    )
    w_up, w_down = gathered(shard)

    spread = call(
        spread_kernel,
        shape((cores, ny, nx, nz * inner, wide), BF16),
        got.reshape(count, wide),
        scratch=(pltpu.VMEM((cores, nx, nz * inner, wide), F32),),
    )
    rows = lax.all_to_all(
        spread.reshape(cores * ny, nx * nz * inner, wide), (CORE, TY), 0, 0, tiled=True
    )
    hidden = call(
        up_kernel,
        shape((ny, 2 * group, nx * units), BF16),
        rows.reshape(cores, tp, nz * inner, wide),
        norm_gain.astype(F32).reshape(1, full),
        w_up,
        flops=1 << 28,
        scratch=(pltpu.VMEM((2 * group, full), F32), pltpu.VMEM((2 * group, full), BF16)),
    )
    hidden = lax.all_to_all(hidden, TY, 0, 0, tiled=True)
    out = call(
        functools.partial(down_kernel, cores),
        shape((count, wide), BF16),
        hidden,
        w_down,
        flops=1 << 27,
        scratch=(pltpu.VMEM((nz // 2, 2, cores, nx // 2, 2 * inner, wide), F32),),
    )

    back = lax.all_to_all(
        out.reshape(ep * nx, inner, wide), (Z, CORE, TX), 0, 0, tiled=True
    )
    first, rest = call(
        mix_kernel,
        [shape((2 * count, tok_rows), BF16)] * 2,
        place,
        route_weight.astype(F32).T,
    )
    combined = call(
        combine_kernel, shape((width, tok_rows), BF16), back.reshape(count, wide), first, rest
    )
    return combined.T


def solution(mesh):
    devices = mesh.devices.reshape(mesh.shape["ep"] // 2, 2, 4, 4)
    split = Mesh(devices, (Z, CORE, TY, TX))
    in_specs = (
        P(EP, TP),
        P(),
        P(EP, None, TP),
        P(EP, None, TP),
        P(EP, None, TP),
        P(EP, None),
        P(EP, None),
    )
    return jax.shard_map(body, mesh=split, in_specs=in_specs, out_specs=P(EP, TP), check_vma=False)
```

```python
import functools

import jax
import jax.numpy as jnp
from jax import lax
from jax.experimental import pallas as pl
from jax.experimental.pallas import tpu as pltpu
from jax.sharding import Mesh
from jax.sharding import PartitionSpec as P


Z, CORE, TY, TX = "z", "core", "ty", "tx"
EP, TP = (Z, CORE), (TY, TX)
EPSILON = 1e-06
ALPHA = 1.702
LIMIT = 7.0
BF16, F32, I32 = jnp.bfloat16, jnp.float32, jnp.int32
NT = (((1,), (1,)), ((), ()))


def iota(shape, dim):
    return lax.broadcasted_iota(I32, shape, dim)


def dot(a, b):
    return jnp.dot(a, b, preferred_element_type=F32)


def dot_nt(a, b):
    return lax.dot_general(a, b, NT, preferred_element_type=F32)


def ones_where(mask):
    return jnp.where(mask, 1.0, 0.0).astype(BF16)


def quads(first, second):
    half = first.shape[1] // 2
    top = iota(first.shape, 1) < half
    return (
        jnp.where(top, first, pltpu.roll(second, half, 1)),
        jnp.where(top, pltpu.roll(first, half, 1), second),
    )


def halves(first, second):
    wide = first.shape[1] // 2
    left = iota(first.shape, 1) < wide
    return (
        jnp.where(left, first, pltpu.roll(second, wide, 1)),
        jnp.where(left, pltpu.roll(first, wide, 1), second),
    )


def prep_kernel(
    sizes, ids_hbm, tokens_hbm, gate_hbm, up_hbm, down_hbm, sent_ref, place_ref, shard_ref,
    ids_ref, tokens_ref, sems
):
    nz, cores, nx = sizes
    small = [(ids_hbm, ids_ref), (tokens_hbm, tokens_ref)]
    large = [(w, shard_ref.at[i]) for i, w in enumerate((gate_hbm, up_hbm, down_hbm))]
    copies = [pltpu.make_async_copy(a, b, sems.at[i]) for i, (a, b) in enumerate(small + large)]
    for copy in copies:
        copy.start()
    top, toks = ids_ref.shape
    count, _ = sent_ref.shape
    experts = nz * cores
    half = count // experts
    inner = half // nx
    earlier = ones_where(iota((toks, toks), 0) < iota((toks, toks), 1))
    expert = iota((experts, toks), 0)
    copies[0].wait()
    ids = ids_ref[...]
    picks = [expert == ids[k : k + 1] for k in range(top)]
    named = picks[0]
    for pick in picks[1:]:
        named = named | pick
    before = dot(ones_where(named), earlier)
    lane = iota((2 * count, toks), 0)
    hit = None
    for k in range(top):
        slot = jnp.sum(jnp.where(picks[k], before, 0.0), axis=0, keepdims=True).astype(I32)
        low, high = slot & (half - 1), jnp.where(slot >= half, count, 0)
        owner = ids[k : k + 1]
        place_ref[k : k + 1] = owner * half + low + high
        x, r = low >> (inner.bit_length() - 1), low & (inner - 1)
        z, core = owner >> (cores.bit_length() - 1), owner & (cores - 1)
        place = ((z * nx + x) * cores + core) * inner + r + high
        hit = (lane == place) if hit is None else hit | (lane == place)
    select = ones_where(hit)
    copies[1].wait()
    tokens = tokens_ref[...].astype(F32)
    zero = jnp.zeros_like(tokens)
    both = jnp.concatenate(
        [jnp.concatenate([tokens, zero], 1), jnp.concatenate([zero, tokens], 1)], 0
    ).astype(BF16)
    both_select = jnp.concatenate([select[:count], select[count:]], 1)
    sent_ref[...] = dot_nt(both_select, both).astype(BF16)
    for copy in copies[2:]:
        copy.wait()


def mix_kernel(place_ref, weight_ref, gain_ref, first_ref, rest_ref, gain_out_ref):
    gain_out_ref[...] = gain_ref[...]
    count, toks = first_ref.shape
    lane = iota((count, toks), 0)
    mix = jnp.zeros((count, toks), F32)
    for k in range(place_ref.shape[0]):
        mix = mix + jnp.where(lane == place_ref[k : k + 1], weight_ref[k : k + 1], 0.0)
    first = mix.astype(BF16)
    first_ref[...] = first
    rest_ref[...] = (mix - first.astype(F32)).astype(BF16)


def spread_kernel(got_ref, out_ref, turned):
    cores, copies, nx, rows, wide = out_ref.shape
    got = got_ref[...].astype(F32).reshape(-1, 2, nx, 8, wide)
    for x in range(nx):
        for core, part in enumerate(quads(got[:, 0, x], got[:, 1, x])):
            turned[core, x] = part.reshape(rows, wide)
    for core in range(cores):
        for x in range(nx):
            part = turned[core, x].astype(BF16)
            for c in range(copies):
                out_ref[core, c, x] = part


def up_kernel(rows_ref, gain_ref, weights_ref, out_ref, whole, normed):
    cores, pieces, part, wide = rows_ref.shape
    group = cores * part
    full = normed.shape[1]
    squares = [jnp.zeros((group, wide), F32) for _ in range(2)]
    for j in range(pieces // 2):
        even, odd = (
            jnp.concatenate([rows_ref[c, 2 * j + i].astype(F32) for c in range(cores)], 0)
            for i in range(2)
        )
        pair = halves(even, odd)
        for h in range(2):
            whole[h * group : (h + 1) * group, j * wide : (j + 1) * wide] = pair[h]
            squares[h] = squares[h] + pair[h] * pair[h]
    for h in range(2):
        mean = jnp.sum(squares[h], axis=1, keepdims=True) / full
        inverse = lax.rsqrt(mean + EPSILON)
        rows = slice(h * group, (h + 1) * group)
        normed[rows] = (whole[rows] * inverse * gain_ref[...]).astype(BF16)
    nx, _, units, _ = weights_ref.shape
    w_gate = weights_ref[:, 0].reshape(nx * units, full)
    w_up = weights_ref[:, 1].reshape(nx * units, full)
    gate = jnp.minimum(dot_nt(normed[...], w_gate), LIMIT)
    up = jnp.clip(dot_nt(normed[...], w_up), -LIMIT, LIMIT)
    hidden = ((up + 1.0) * gate * jax.nn.sigmoid(ALPHA * gate)).astype(BF16)
    for c in range(out_ref.shape[0]):
        out_ref[c] = hidden


def down_kernel(cores, hidden_ref, weights_ref, out_ref, turned):
    ny, rows, units = hidden_ref.shape
    nx, width, full = weights_ref.shape
    w_down = weights_ref[...].reshape(nx * width, full)
    total = dot_nt(hidden_ref[0], w_down[:, :units])
    for y in range(1, ny):
        total = total + dot_nt(hidden_ref[y], w_down[:, y * units : (y + 1) * units])
    group = rows // 2
    pieces = []
    for j in range(nx // 2):
        lanes = slice(2 * j * width, 2 * (j + 1) * width)
        pieces += halves(total[:group, lanes], total[group:, lanes])
    for j in range(nx // 2):
        first, second = (p.reshape(-1, 8, 2 * width) for p in pieces[2 * j : 2 * j + 2])
        for odd, part in enumerate(quads(first, second)):
            part = part.reshape(cores, -1, 8, 2 * width)
            for core in range(cores):
                turned[:, odd, core, j] = part[core]
    out_ref[...] = turned[...].reshape(out_ref.shape).astype(BF16)


def combine_kernel(back_ref, first_ref, rest_ref, out_ref):
    count = back_ref.shape[0]
    width = out_ref.shape[0]
    back = back_ref[...].astype(F32).T.astype(BF16)
    total = jnp.zeros(out_ref.shape, F32)
    for h in range(2):
        piece = back[h * width : (h + 1) * width]
        for part in (first_ref, rest_ref):
            total = total + dot(piece, part[h * count : (h + 1) * count])
    out_ref[...] = total.astype(BF16)


def call(kernel, out_shapes, *args, flops=1 << 24, scratch=(), space=pltpu.VMEM, vmem=16):
    single = not isinstance(out_shapes, list)
    outs = [out_shapes] if single else out_shapes
    out_specs = [pl.BlockSpec(memory_space=pltpu.VMEM)] * len(outs)
    return pl.pallas_call(
        kernel,
        out_shape=out_shapes,
        in_specs=[pl.BlockSpec(memory_space=space)] * len(args),
        out_specs=out_specs[0] if single else out_specs,
        scratch_shapes=list(scratch),
        cost_estimate=pl.CostEstimate(flops=flops, bytes_accessed=1 << 20, transcendentals=0),
        compiler_params=pltpu.CompilerParams(vmem_limit_bytes=vmem << 20),
    )(*args)


def set_at(whole, piece, index):
    return lax.dynamic_update_slice_in_dim(whole, piece[None], index, 0)


def gathered(shard):
    count = lax.axis_size(TX)
    me = lax.axis_index(TX)
    near, after = ([(i, (i + hop) % count) for i in range(count)] for hop in (1, count - 1))
    left = lax.ppermute(shard, TX, near)
    right = lax.ppermute(shard, TX, after)
    far_up = lax.ppermute(left[:2], TX, near)
    far_down = lax.ppermute(right[2], TX, after)
    up = jnp.zeros((count, 2) + shard.shape[1:], shard.dtype)
    down = jnp.zeros((count,) + shard.shape[1:], shard.dtype)
    before, behind, across = (lax.rem(me + hop, count) for hop in (count - 1, 1, count - 2))
    for piece, source in ((left, before), (right, behind), (shard, me)):
        up = set_at(up, piece[:2], source)
    up = set_at(up, far_up, across)
    for piece, source in ((left, before), (right, behind), (shard, me)):
        down = set_at(down, piece[2], source)
    down = set_at(down, far_down, across)
    return up, down


def body(tokens, norm_gain, gate_weight, up_weight, down_weight, expert_ids, route_weight):
    tok_rows, top = expert_ids.shape
    width = tokens.shape[1]
    full = norm_gain.shape[0]
    nz, cores, ny, nx = (lax.axis_size(axis) for axis in (Z, CORE, TY, TX))
    ep, tp = nz * cores, ny * nx
    units = gate_weight.shape[2]
    half = tok_rows * top // ep
    inner = half // nx
    count, wide = ep * half, 2 * width
    group = count // nx
    shape = jax.ShapeDtypeStruct

    sent, place, shard = call(
        functools.partial(prep_kernel, (nz, cores, nx)),
        [
            shape((count, wide), BF16),
            shape((top, tok_rows), I32),
            shape((3, units, full), BF16),
        ],
        expert_ids.T,
        tokens.T,
        gate_weight[0].T,
        up_weight[0].T,
        down_weight[0].T,
        scratch=(
            pltpu.VMEM((top, tok_rows), I32),
            pltpu.VMEM((width, tok_rows), BF16),
            pltpu.SemaphoreType.DMA((5,)),
        ),
        space=pltpu.HBM,
        vmem=62,
    )
    got = lax.all_to_all(
        sent.reshape(nz * nx, cores * inner, wide), (Z, TX), 0, 0, tiled=True
    )
    w_up, w_down = gathered(shard)

    spread = call(
        spread_kernel,
        shape((cores, ny, nx, nz * inner, wide), BF16),
        got.reshape(count, wide),
        scratch=(pltpu.VMEM((cores, nx, nz * inner, wide), F32),),
    )
    rows = lax.all_to_all(
        spread.reshape(cores * ny, nx * nz * inner, wide), (CORE, TY), 0, 0, tiled=True
    )
    first, rest, gain = call(
        mix_kernel,
        [shape((2 * count, tok_rows), BF16)] * 2 + [shape((1, full), F32)],
        place,
        route_weight.astype(F32).T,
        norm_gain.astype(F32).reshape(1, full),
    )
    hidden = call(
        up_kernel,
        shape((ny, 2 * group, nx * units), BF16),
        rows.reshape(cores, tp, nz * inner, wide),
        gain,
        w_up,
        flops=1 << 28,
        scratch=(pltpu.VMEM((2 * group, full), F32), pltpu.VMEM((2 * group, full), BF16)),
    )
    hidden = lax.all_to_all(hidden, TY, 0, 0, tiled=True)
    out = call(
        functools.partial(down_kernel, cores),
        shape((count, wide), BF16),
        hidden,
        w_down,
        flops=1 << 27,
        scratch=(pltpu.VMEM((nz // 2, 2, cores, nx // 2, 2 * inner, wide), F32),),
    )

    back = lax.all_to_all(
        out.reshape(ep * nx, inner, wide), (Z, CORE, TX), 0, 0, tiled=True
    )
    combined = call(
        combine_kernel, shape((width, tok_rows), BF16), back.reshape(count, wide), first, rest
    )
    return combined.T


def solution(mesh):
    devices = mesh.devices.reshape(mesh.shape["ep"] // 2, 2, 4, 4)
    split = Mesh(devices, (Z, CORE, TY, TX))
    in_specs = (
        P(EP, TP),
        P(),
        P(EP, None, TP),
        P(EP, None, TP),
        P(EP, None, TP),
        P(EP, None),
        P(EP, None),
    )
    return jax.shard_map(body, mesh=split, in_specs=in_specs, out_specs=P(EP, TP), check_vma=False)
```

```python
import functools

import jax
import jax.numpy as jnp
from jax import lax
from jax.experimental import pallas as pl
from jax.experimental.pallas import tpu as pltpu
from jax.sharding import Mesh
from jax.sharding import PartitionSpec as P


Z, CORE, TY, TX = "z", "core", "ty", "tx"
EP, TP = (Z, CORE), (TY, TX)
EPSILON = 1e-06
ALPHA = 1.702
LIMIT = 7.0
BF16, F32, I32 = jnp.bfloat16, jnp.float32, jnp.int32
NT = (((1,), (1,)), ((), ()))


def iota(shape, dim):
    return lax.broadcasted_iota(I32, shape, dim)


def dot(a, b):
    return jnp.dot(a, b, preferred_element_type=F32)


def dot_nt(a, b):
    return lax.dot_general(a, b, NT, preferred_element_type=F32)


def ones_where(mask):
    return jnp.where(mask, 1.0, 0.0).astype(BF16)


def quads(first, second):
    half = first.shape[1] // 2
    top = iota(first.shape, 1) < half
    return (
        jnp.where(top, first, pltpu.roll(second, half, 1)),
        jnp.where(top, pltpu.roll(first, half, 1), second),
    )


def halves(first, second):
    wide = first.shape[1] // 2
    left = iota(first.shape, 1) < wide
    return (
        jnp.where(left, first, pltpu.roll(second, wide, 1)),
        jnp.where(left, pltpu.roll(first, wide, 1), second),
    )


def prep_kernel(
    sizes, ids_hbm, tokens_hbm, gate_hbm, up_hbm, down_hbm, sent_ref, place_ref, shard_ref,
    pair_ref, ids_ref, tokens_ref, sems
):
    nz, cores, nx = sizes
    small = [(ids_hbm, ids_ref), (tokens_hbm, tokens_ref)]
    large = [(w, shard_ref.at[i]) for i, w in enumerate((gate_hbm, up_hbm, down_hbm))]
    large += [(w, pair_ref.at[i]) for i, w in enumerate((gate_hbm, up_hbm))]
    copies = [pltpu.make_async_copy(a, b, sems.at[i]) for i, (a, b) in enumerate(small + large)]
    for copy in copies:
        copy.start()
    top, toks = ids_ref.shape
    count, _ = sent_ref.shape
    experts = nz * cores
    half = count // experts
    inner = half // nx
    earlier = ones_where(iota((toks, toks), 0) < iota((toks, toks), 1))
    expert = iota((experts, toks), 0)
    copies[0].wait()
    ids = ids_ref[...]
    picks = [expert == ids[k : k + 1] for k in range(top)]
    named = picks[0]
    for pick in picks[1:]:
        named = named | pick
    before = dot(ones_where(named), earlier)
    lane = iota((2 * count, toks), 0)
    hit = None
    for k in range(top):
        slot = jnp.sum(jnp.where(picks[k], before, 0.0), axis=0, keepdims=True).astype(I32)
        low, high = slot & (half - 1), jnp.where(slot >= half, count, 0)
        owner = ids[k : k + 1]
        place_ref[k : k + 1] = owner * half + low + high
        x, r = low >> (inner.bit_length() - 1), low & (inner - 1)
        z, core = owner >> (cores.bit_length() - 1), owner & (cores - 1)
        place = ((z * nx + x) * cores + core) * inner + r + high
        hit = (lane == place) if hit is None else hit | (lane == place)
    select = ones_where(hit)
    copies[1].wait()
    tokens = tokens_ref[...].astype(F32)
    zero = jnp.zeros_like(tokens)
    both = jnp.concatenate(
        [jnp.concatenate([tokens, zero], 1), jnp.concatenate([zero, tokens], 1)], 0
    ).astype(BF16)
    both_select = jnp.concatenate([select[:count], select[count:]], 1)
    sent_ref[...] = dot_nt(both_select, both).astype(BF16)
    for copy in copies[2:]:
        copy.wait()


def mix_kernel(place_ref, weight_ref, gain_ref, first_ref, rest_ref, gain_out_ref):
    gain_out_ref[...] = gain_ref[...]
    count, toks = first_ref.shape
    lane = iota((count, toks), 0)
    mix = jnp.zeros((count, toks), F32)
    for k in range(place_ref.shape[0]):
        mix = mix + jnp.where(lane == place_ref[k : k + 1], weight_ref[k : k + 1], 0.0)
    first = mix.astype(BF16)
    first_ref[...] = first
    rest_ref[...] = (mix - first.astype(F32)).astype(BF16)


def spread_kernel(got_ref, out_ref, turned):
    cores, copies, nx, rows, wide = out_ref.shape
    got = got_ref[...].astype(F32).reshape(-1, 2, nx, 8, wide)
    for x in range(nx):
        for core, part in enumerate(quads(got[:, 0, x], got[:, 1, x])):
            turned[core, x] = part.reshape(rows, wide)
    for core in range(cores):
        for x in range(nx):
            part = turned[core, x].astype(BF16)
            for c in range(copies):
                out_ref[core, c, x] = part


def up_kernel(rows_ref, gain_ref, weights_ref, out_ref, whole, normed):
    cores, pieces, part, wide = rows_ref.shape
    group = cores * part
    full = normed.shape[1]
    squares = [jnp.zeros((group, wide), F32) for _ in range(2)]
    for j in range(pieces // 2):
        even, odd = (
            jnp.concatenate([rows_ref[c, 2 * j + i].astype(F32) for c in range(cores)], 0)
            for i in range(2)
        )
        pair = halves(even, odd)
        for h in range(2):
            whole[h * group : (h + 1) * group, j * wide : (j + 1) * wide] = pair[h]
            squares[h] = squares[h] + pair[h] * pair[h]
    for h in range(2):
        mean = jnp.sum(squares[h], axis=1, keepdims=True) / full
        inverse = lax.rsqrt(mean + EPSILON)
        rows = slice(h * group, (h + 1) * group)
        normed[rows] = (whole[rows] * inverse * gain_ref[...]).astype(BF16)
    nx, _, units, _ = weights_ref.shape
    w_gate = weights_ref[:, 0].reshape(nx * units, full)
    w_up = weights_ref[:, 1].reshape(nx * units, full)
    gate = jnp.minimum(dot_nt(normed[...], w_gate), LIMIT)
    up = jnp.clip(dot_nt(normed[...], w_up), -LIMIT, LIMIT)
    hidden = ((up + 1.0) * gate * jax.nn.sigmoid(ALPHA * gate)).astype(BF16)
    for c in range(out_ref.shape[0]):
        out_ref[c] = hidden


def down_kernel(cores, hidden_ref, weights_ref, out_ref, turned):
    ny, rows, units = hidden_ref.shape
    nx, width, full = weights_ref.shape
    w_down = weights_ref[...].reshape(nx * width, full)
    total = dot_nt(hidden_ref[0], w_down[:, :units])
    for y in range(1, ny):
        total = total + dot_nt(hidden_ref[y], w_down[:, y * units : (y + 1) * units])
    group = rows // 2
    pieces = []
    for j in range(nx // 2):
        lanes = slice(2 * j * width, 2 * (j + 1) * width)
        pieces += halves(total[:group, lanes], total[group:, lanes])
    for j in range(nx // 2):
        first, second = (p.reshape(-1, 8, 2 * width) for p in pieces[2 * j : 2 * j + 2])
        for odd, part in enumerate(quads(first, second)):
            part = part.reshape(cores, -1, 8, 2 * width)
            for core in range(cores):
                turned[:, odd, core, j] = part[core]
    out_ref[...] = turned[...].reshape(out_ref.shape).astype(BF16)


def combine_kernel(back_ref, first_ref, rest_ref, out_ref):
    count = back_ref.shape[0]
    width = out_ref.shape[0]
    back = back_ref[...].astype(F32).T.astype(BF16)
    total = jnp.zeros(out_ref.shape, F32)
    for h in range(2):
        piece = back[h * width : (h + 1) * width]
        for part in (first_ref, rest_ref):
            total = total + dot(piece, part[h * count : (h + 1) * count])
    out_ref[...] = total.astype(BF16)


def call(kernel, out_shapes, *args, flops=1 << 24, scratch=(), space=pltpu.VMEM, vmem=16):
    single = not isinstance(out_shapes, list)
    outs = [out_shapes] if single else out_shapes
    out_specs = [pl.BlockSpec(memory_space=pltpu.VMEM)] * len(outs)
    return pl.pallas_call(
        kernel,
        out_shape=out_shapes,
        in_specs=[pl.BlockSpec(memory_space=space)] * len(args),
        out_specs=out_specs[0] if single else out_specs,
        scratch_shapes=list(scratch),
        cost_estimate=pl.CostEstimate(flops=flops, bytes_accessed=1 << 20, transcendentals=0),
        compiler_params=pltpu.CompilerParams(vmem_limit_bytes=vmem << 20),
    )(*args)


def set_at(whole, piece, index):
    return lax.dynamic_update_slice_in_dim(whole, piece[None], index, 0)


def gathered(shard, pair):
    count = lax.axis_size(TX)
    me = lax.axis_index(TX)
    near, far, after = (
        [(i, (i + hop) % count) for i in range(count)] for hop in (1, count - 2, count - 1)
    )
    right = lax.ppermute(shard, TX, after)
    far_up = lax.ppermute(pair, TX, far)
    left = lax.ppermute(shard, TX, near)
    far_down = lax.ppermute(right[2], TX, after)
    up = jnp.zeros((count, 2) + shard.shape[1:], shard.dtype)
    down = jnp.zeros((count,) + shard.shape[1:], shard.dtype)
    before, behind, across = (lax.rem(me + hop, count) for hop in (count - 1, 1, count - 2))
    for piece, source in ((left, before), (right, behind), (shard, me)):
        up = set_at(up, piece[:2], source)
    up = set_at(up, far_up, across)
    for piece, source in ((right, behind), (left, before), (shard, me)):
        down = set_at(down, piece[2], source)
    down = set_at(down, far_down, across)
    return up, down


def body(tokens, norm_gain, gate_weight, up_weight, down_weight, expert_ids, route_weight):
    tok_rows, top = expert_ids.shape
    width = tokens.shape[1]
    full = norm_gain.shape[0]
    nz, cores, ny, nx = (lax.axis_size(axis) for axis in (Z, CORE, TY, TX))
    ep, tp = nz * cores, ny * nx
    units = gate_weight.shape[2]
    half = tok_rows * top // ep
    inner = half // nx
    count, wide = ep * half, 2 * width
    group = count // nx
    shape = jax.ShapeDtypeStruct

    sent, place, shard, pair = call(
        functools.partial(prep_kernel, (nz, cores, nx)),
        [
            shape((count, wide), BF16),
            shape((top, tok_rows), I32),
            shape((3, units, full), BF16),
            shape((2, units, full), BF16),
        ],
        expert_ids.T,
        tokens.T,
        gate_weight[0].T,
        up_weight[0].T,
        down_weight[0].T,
        scratch=(
            pltpu.VMEM((top, tok_rows), I32),
            pltpu.VMEM((width, tok_rows), BF16),
            pltpu.SemaphoreType.DMA((7,)),
        ),
        space=pltpu.HBM,
        vmem=62,
    )
    got = lax.all_to_all(
        sent.reshape(nz * nx, cores * inner, wide), (Z, TX), 0, 0, tiled=True
    )
    w_up, w_down = gathered(shard, pair)

    spread = call(
        spread_kernel,
        shape((cores, ny, nx, nz * inner, wide), BF16),
        got.reshape(count, wide),
        scratch=(pltpu.VMEM((cores, nx, nz * inner, wide), F32),),
    )
    rows = lax.all_to_all(
        spread.reshape(cores * ny, nx * nz * inner, wide), (CORE, TY), 0, 0, tiled=True
    )
    first, rest, gain = call(
        mix_kernel,
        [shape((2 * count, tok_rows), BF16)] * 2 + [shape((1, full), F32)],
        place,
        route_weight.astype(F32).T,
        norm_gain.astype(F32).reshape(1, full),
    )
    hidden = call(
        up_kernel,
        shape((ny, 2 * group, nx * units), BF16),
        rows.reshape(cores, tp, nz * inner, wide),
        gain,
        w_up,
        flops=1 << 28,
        scratch=(pltpu.VMEM((2 * group, full), F32), pltpu.VMEM((2 * group, full), BF16)),
    )
    hidden = lax.all_to_all(hidden, TY, 0, 0, tiled=True)
    out = call(
        functools.partial(down_kernel, cores),
        shape((count, wide), BF16),
        hidden,
        w_down,
        flops=1 << 27,
        scratch=(pltpu.VMEM((nz // 2, 2, cores, nx // 2, 2 * inner, wide), F32),),
    )

    back = lax.all_to_all(
        out.reshape(ep * nx, inner, wide), (Z, CORE, TX), 0, 0, tiled=True
    )
    combined = call(
        combine_kernel, shape((width, tok_rows), BF16), back.reshape(count, wide), first, rest
    )
    return combined.T


def solution(mesh):
    devices = mesh.devices.reshape(mesh.shape["ep"] // 2, 2, 4, 4)
    split = Mesh(devices, (Z, CORE, TY, TX))
    in_specs = (
        P(EP, TP),
        P(),
        P(EP, None, TP),
        P(EP, None, TP),
        P(EP, None, TP),
        P(EP, None),
        P(EP, None),
    )
    return jax.shard_map(body, mesh=split, in_specs=in_specs, out_specs=P(EP, TP), check_vma=False)
```

```python
import functools

import jax
import jax.numpy as jnp
from jax import lax
from jax.experimental import pallas as pl
from jax.experimental.pallas import tpu as pltpu
from jax.sharding import Mesh
from jax.sharding import PartitionSpec as P


Z, CORE, TY, TX = "z", "core", "ty", "tx"
EP, TP = (Z, CORE), (TY, TX)
EPSILON = 1e-06
ALPHA = 1.702
LIMIT = 7.0
BF16, F32, I32 = jnp.bfloat16, jnp.float32, jnp.int32
NT = (((1,), (1,)), ((), ()))


def iota(shape, dim):
    return lax.broadcasted_iota(I32, shape, dim)


def dot(a, b):
    return jnp.dot(a, b, preferred_element_type=F32)


def dot_nt(a, b):
    return lax.dot_general(a, b, NT, preferred_element_type=F32)


def ones_where(mask):
    return jnp.where(mask, 1.0, 0.0).astype(BF16)


def quads(first, second):
    half = first.shape[1] // 2
    top = iota(first.shape, 1) < half
    return (
        jnp.where(top, first, pltpu.roll(second, half, 1)),
        jnp.where(top, pltpu.roll(first, half, 1), second),
    )


def halves(first, second):
    wide = first.shape[1] // 2
    left = iota(first.shape, 1) < wide
    return (
        jnp.where(left, first, pltpu.roll(second, wide, 1)),
        jnp.where(left, pltpu.roll(first, wide, 1), second),
    )


def prep_kernel(
    sizes, ids_hbm, tokens_hbm, gate_hbm, up_hbm, down_hbm, sent_ref, place_ref, shard_ref,
    gate_ref, ids_ref, tokens_ref, sems
):
    nz, cores, nx = sizes
    small = [(ids_hbm, ids_ref), (tokens_hbm, tokens_ref)]
    large = [(w, shard_ref.at[i]) for i, w in enumerate((gate_hbm, up_hbm, down_hbm))]
    large += [(gate_hbm, gate_ref)]
    copies = [pltpu.make_async_copy(a, b, sems.at[i]) for i, (a, b) in enumerate(small + large)]
    for copy in copies:
        copy.start()
    top, toks = ids_ref.shape
    count, _ = sent_ref.shape
    experts = nz * cores
    half = count // experts
    inner = half // nx
    earlier = ones_where(iota((toks, toks), 0) < iota((toks, toks), 1))
    expert = iota((experts, toks), 0)
    copies[0].wait()
    ids = ids_ref[...]
    picks = [expert == ids[k : k + 1] for k in range(top)]
    named = picks[0]
    for pick in picks[1:]:
        named = named | pick
    before = dot(ones_where(named), earlier)
    lane = iota((2 * count, toks), 0)
    hit = None
    for k in range(top):
        slot = jnp.sum(jnp.where(picks[k], before, 0.0), axis=0, keepdims=True).astype(I32)
        low, high = slot & (half - 1), jnp.where(slot >= half, count, 0)
        owner = ids[k : k + 1]
        place_ref[k : k + 1] = owner * half + low + high
        x, r = low >> (inner.bit_length() - 1), low & (inner - 1)
        z, core = owner >> (cores.bit_length() - 1), owner & (cores - 1)
        place = ((z * nx + x) * cores + core) * inner + r + high
        hit = (lane == place) if hit is None else hit | (lane == place)
    select = ones_where(hit)
    copies[1].wait()
    tokens = tokens_ref[...].astype(F32)
    zero = jnp.zeros_like(tokens)
    both = jnp.concatenate(
        [jnp.concatenate([tokens, zero], 1), jnp.concatenate([zero, tokens], 1)], 0
    ).astype(BF16)
    both_select = jnp.concatenate([select[:count], select[count:]], 1)
    sent_ref[...] = dot_nt(both_select, both).astype(BF16)
    for copy in copies[2:]:
        copy.wait()


def mix_kernel(place_ref, weight_ref, gain_ref, first_ref, rest_ref, gain_out_ref):
    gain_out_ref[...] = gain_ref[...]
    count, toks = first_ref.shape
    lane = iota((count, toks), 0)
    mix = jnp.zeros((count, toks), F32)
    for k in range(place_ref.shape[0]):
        mix = mix + jnp.where(lane == place_ref[k : k + 1], weight_ref[k : k + 1], 0.0)
    first = mix.astype(BF16)
    first_ref[...] = first
    rest_ref[...] = (mix - first.astype(F32)).astype(BF16)


def spread_kernel(got_ref, out_ref, turned):
    cores, copies, nx, rows, wide = out_ref.shape
    got = got_ref[...].astype(F32).reshape(-1, 2, nx, 8, wide)
    for x in range(nx):
        for core, part in enumerate(quads(got[:, 0, x], got[:, 1, x])):
            turned[core, x] = part.reshape(rows, wide)
    for core in range(cores):
        for x in range(nx):
            part = turned[core, x].astype(BF16)
            for c in range(copies):
                out_ref[core, c, x] = part


def up_kernel(rows_ref, gain_ref, weights_ref, out_ref, whole, normed):
    cores, pieces, part, wide = rows_ref.shape
    group = cores * part
    full = normed.shape[1]
    squares = [jnp.zeros((group, wide), F32) for _ in range(2)]
    for j in range(pieces // 2):
        even, odd = (
            jnp.concatenate([rows_ref[c, 2 * j + i].astype(F32) for c in range(cores)], 0)
            for i in range(2)
        )
        pair = halves(even, odd)
        for h in range(2):
            whole[h * group : (h + 1) * group, j * wide : (j + 1) * wide] = pair[h]
            squares[h] = squares[h] + pair[h] * pair[h]
    for h in range(2):
        mean = jnp.sum(squares[h], axis=1, keepdims=True) / full
        inverse = lax.rsqrt(mean + EPSILON)
        rows = slice(h * group, (h + 1) * group)
        normed[rows] = (whole[rows] * inverse * gain_ref[...]).astype(BF16)
    nx, _, units, _ = weights_ref.shape
    w_gate = weights_ref[:, 0].reshape(nx * units, full)
    w_up = weights_ref[:, 1].reshape(nx * units, full)
    gate = jnp.minimum(dot_nt(normed[...], w_gate), LIMIT)
    up = jnp.clip(dot_nt(normed[...], w_up), -LIMIT, LIMIT)
    hidden = ((up + 1.0) * gate * jax.nn.sigmoid(ALPHA * gate)).astype(BF16)
    for c in range(out_ref.shape[0]):
        out_ref[c] = hidden


def down_kernel(cores, hidden_ref, weights_ref, out_ref, turned):
    ny, rows, units = hidden_ref.shape
    nx, width, full = weights_ref.shape
    w_down = weights_ref[...].reshape(nx * width, full)
    total = dot_nt(hidden_ref[0], w_down[:, :units])
    for y in range(1, ny):
        total = total + dot_nt(hidden_ref[y], w_down[:, y * units : (y + 1) * units])
    group = rows // 2
    pieces = []
    for j in range(nx // 2):
        lanes = slice(2 * j * width, 2 * (j + 1) * width)
        pieces += halves(total[:group, lanes], total[group:, lanes])
    for j in range(nx // 2):
        first, second = (p.reshape(-1, 8, 2 * width) for p in pieces[2 * j : 2 * j + 2])
        for odd, part in enumerate(quads(first, second)):
            part = part.reshape(cores, -1, 8, 2 * width)
            for core in range(cores):
                turned[:, odd, core, j] = part[core]
    out_ref[...] = turned[...].reshape(out_ref.shape).astype(BF16)


def combine_kernel(back_ref, first_ref, rest_ref, out_ref):
    count = back_ref.shape[0]
    width = out_ref.shape[0]
    back = back_ref[...].astype(F32).T.astype(BF16)
    total = jnp.zeros(out_ref.shape, F32)
    for h in range(2):
        piece = back[h * width : (h + 1) * width]
        for part in (first_ref, rest_ref):
            total = total + dot(piece, part[h * count : (h + 1) * count])
    out_ref[...] = total.astype(BF16)


def call(kernel, out_shapes, *args, flops=1 << 24, scratch=(), space=pltpu.VMEM, vmem=16):
    single = not isinstance(out_shapes, list)
    outs = [out_shapes] if single else out_shapes
    out_specs = [pl.BlockSpec(memory_space=pltpu.VMEM)] * len(outs)
    return pl.pallas_call(
        kernel,
        out_shape=out_shapes,
        in_specs=[pl.BlockSpec(memory_space=space)] * len(args),
        out_specs=out_specs[0] if single else out_specs,
        scratch_shapes=list(scratch),
        cost_estimate=pl.CostEstimate(flops=flops, bytes_accessed=1 << 20, transcendentals=0),
        compiler_params=pltpu.CompilerParams(vmem_limit_bytes=vmem << 20),
    )(*args)


def set_at(whole, piece, index):
    return lax.dynamic_update_slice_in_dim(whole, piece[None], index, 0)


def gathered(shard, gate):
    count = lax.axis_size(TX)
    me = lax.axis_index(TX)
    near, far, after = (
        [(i, (i + hop) % count) for i in range(count)] for hop in (1, count - 2, count - 1)
    )
    right = lax.ppermute(shard, TX, after)
    far_gate = lax.ppermute(gate, TX, far)
    left = lax.ppermute(shard, TX, near)
    far_up = lax.ppermute(right[1], TX, after)
    far_down = lax.ppermute(left[2], TX, near)
    up = jnp.zeros((count, 2) + shard.shape[1:], shard.dtype)
    down = jnp.zeros((count,) + shard.shape[1:], shard.dtype)
    before, behind, across = (lax.rem(me + hop, count) for hop in (count - 1, 1, count - 2))
    for piece, source in ((right, behind), (left, before), (shard, me)):
        up = set_at(up, piece[:2], source)
    for half, piece in enumerate((far_gate, far_up)):
        up = lax.dynamic_update_slice(up, piece[None, None], (across, half, 0, 0))
    for piece, source in ((right, behind), (left, before), (shard, me)):
        down = set_at(down, piece[2], source)
    down = set_at(down, far_down, across)
    return up, down


def body(tokens, norm_gain, gate_weight, up_weight, down_weight, expert_ids, route_weight):
    tok_rows, top = expert_ids.shape
    width = tokens.shape[1]
    full = norm_gain.shape[0]
    nz, cores, ny, nx = (lax.axis_size(axis) for axis in (Z, CORE, TY, TX))
    ep, tp = nz * cores, ny * nx
    units = gate_weight.shape[2]
    half = tok_rows * top // ep
    inner = half // nx
    count, wide = ep * half, 2 * width
    group = count // nx
    shape = jax.ShapeDtypeStruct

    sent, place, shard, gate = call(
        functools.partial(prep_kernel, (nz, cores, nx)),
        [
            shape((count, wide), BF16),
            shape((top, tok_rows), I32),
            shape((3, units, full), BF16),
            shape((units, full), BF16),
        ],
        expert_ids.T,
        tokens.T,
        gate_weight[0].T,
        up_weight[0].T,
        down_weight[0].T,
        scratch=(
            pltpu.VMEM((top, tok_rows), I32),
            pltpu.VMEM((width, tok_rows), BF16),
            pltpu.SemaphoreType.DMA((6,)),
        ),
        space=pltpu.HBM,
        vmem=62,
    )
    got = lax.all_to_all(
        sent.reshape(nz * nx, cores * inner, wide), (Z, TX), 0, 0, tiled=True
    )
    w_up, w_down = gathered(shard, gate)

    spread = call(
        spread_kernel,
        shape((cores, ny, nx, nz * inner, wide), BF16),
        got.reshape(count, wide),
        scratch=(pltpu.VMEM((cores, nx, nz * inner, wide), F32),),
    )
    rows = lax.all_to_all(
        spread.reshape(cores * ny, nx * nz * inner, wide), (CORE, TY), 0, 0, tiled=True
    )
    first, rest, gain = call(
        mix_kernel,
        [shape((2 * count, tok_rows), BF16)] * 2 + [shape((1, full), F32)],
        place,
        route_weight.astype(F32).T,
        norm_gain.astype(F32).reshape(1, full),
    )
    hidden = call(
        up_kernel,
        shape((ny, 2 * group, nx * units), BF16),
        rows.reshape(cores, tp, nz * inner, wide),
        gain,
        w_up,
        flops=1 << 28,
        scratch=(pltpu.VMEM((2 * group, full), F32), pltpu.VMEM((2 * group, full), BF16)),
    )
    hidden = lax.all_to_all(hidden, TY, 0, 0, tiled=True)
    out = call(
        functools.partial(down_kernel, cores),
        shape((count, wide), BF16),
        hidden,
        w_down,
        flops=1 << 27,
        scratch=(pltpu.VMEM((nz // 2, 2, cores, nx // 2, 2 * inner, wide), F32),),
    )

    back = lax.all_to_all(
        out.reshape(ep * nx, inner, wide), (Z, CORE, TX), 0, 0, tiled=True
    )
    combined = call(
        combine_kernel, shape((width, tok_rows), BF16), back.reshape(count, wide), first, rest
    )
    return combined.T


def solution(mesh):
    devices = mesh.devices.reshape(mesh.shape["ep"] // 2, 2, 4, 4)
    split = Mesh(devices, (Z, CORE, TY, TX))
    in_specs = (
        P(EP, TP),
        P(),
        P(EP, None, TP),
        P(EP, None, TP),
        P(EP, None, TP),
        P(EP, None),
        P(EP, None),
    )
    return jax.shard_map(body, mesh=split, in_specs=in_specs, out_specs=P(EP, TP), check_vma=False)
```

```python
import functools

import jax
import jax.numpy as jnp
from jax import lax
from jax.experimental import pallas as pl
from jax.experimental.pallas import tpu as pltpu
from jax.sharding import Mesh
from jax.sharding import PartitionSpec as P


Z, CORE, TY, TX = "z", "core", "ty", "tx"
EP, TP = (Z, CORE), (TY, TX)
EPSILON = 1e-06
ALPHA = 1.702
LIMIT = 7.0
BF16, F32, I32 = jnp.bfloat16, jnp.float32, jnp.int32
NT = (((1,), (1,)), ((), ()))


def iota(shape, dim):
    return lax.broadcasted_iota(I32, shape, dim)


def dot(a, b):
    return jnp.dot(a, b, preferred_element_type=F32)


def dot_nt(a, b):
    return lax.dot_general(a, b, NT, preferred_element_type=F32)


def ones_where(mask):
    return jnp.where(mask, 1.0, 0.0).astype(BF16)


def quads(first, second):
    half = first.shape[1] // 2
    top = iota(first.shape, 1) < half
    return (
        jnp.where(top, first, pltpu.roll(second, half, 1)),
        jnp.where(top, pltpu.roll(first, half, 1), second),
    )


def halves(first, second):
    wide = first.shape[1] // 2
    left = iota(first.shape, 1) < wide
    return (
        jnp.where(left, first, pltpu.roll(second, wide, 1)),
        jnp.where(left, pltpu.roll(first, wide, 1), second),
    )


def prep_kernel(
    sizes, ids_hbm, tokens_hbm, gate_hbm, up_hbm, down_hbm, sent_ref, place_ref, shard_ref,
    pair_ref, ids_ref, tokens_ref, sems
):
    nz, cores, nx = sizes
    small = [(ids_hbm, ids_ref), (tokens_hbm, tokens_ref)]
    large = [(w, shard_ref.at[i]) for i, w in enumerate((gate_hbm, up_hbm, down_hbm))]
    large += [(w, pair_ref.at[i]) for i, w in enumerate((gate_hbm, down_hbm))]
    copies = [pltpu.make_async_copy(a, b, sems.at[i]) for i, (a, b) in enumerate(small + large)]
    for copy in copies:
        copy.start()
    top, toks = ids_ref.shape
    count, _ = sent_ref.shape
    experts = nz * cores
    half = count // experts
    inner = half // nx
    earlier = ones_where(iota((toks, toks), 0) < iota((toks, toks), 1))
    expert = iota((experts, toks), 0)
    copies[0].wait()
    ids = ids_ref[...]
    picks = [expert == ids[k : k + 1] for k in range(top)]
    named = picks[0]
    for pick in picks[1:]:
        named = named | pick
    before = dot(ones_where(named), earlier)
    lane = iota((2 * count, toks), 0)
    hit = None
    for k in range(top):
        slot = jnp.sum(jnp.where(picks[k], before, 0.0), axis=0, keepdims=True).astype(I32)
        low, high = slot & (half - 1), jnp.where(slot >= half, count, 0)
        owner = ids[k : k + 1]
        place_ref[k : k + 1] = owner * half + low + high
        x, r = low >> (inner.bit_length() - 1), low & (inner - 1)
        z, core = owner >> (cores.bit_length() - 1), owner & (cores - 1)
        place = ((z * nx + x) * cores + core) * inner + r + high
        hit = (lane == place) if hit is None else hit | (lane == place)
    select = ones_where(hit)
    copies[1].wait()
    tokens = tokens_ref[...].astype(F32)
    zero = jnp.zeros_like(tokens)
    both = jnp.concatenate(
        [jnp.concatenate([tokens, zero], 1), jnp.concatenate([zero, tokens], 1)], 0
    ).astype(BF16)
    both_select = jnp.concatenate([select[:count], select[count:]], 1)
    sent_ref[...] = dot_nt(both_select, both).astype(BF16)
    for copy in copies[2:]:
        copy.wait()


def mix_kernel(place_ref, weight_ref, gain_ref, first_ref, rest_ref, gain_out_ref):
    gain_out_ref[...] = gain_ref[...]
    count, toks = first_ref.shape
    lane = iota((count, toks), 0)
    mix = jnp.zeros((count, toks), F32)
    for k in range(place_ref.shape[0]):
        mix = mix + jnp.where(lane == place_ref[k : k + 1], weight_ref[k : k + 1], 0.0)
    first = mix.astype(BF16)
    first_ref[...] = first
    rest_ref[...] = (mix - first.astype(F32)).astype(BF16)


def spread_kernel(got_ref, out_ref, turned):
    cores, copies, nx, rows, wide = out_ref.shape
    got = got_ref[...].astype(F32).reshape(-1, 2, nx, 8, wide)
    for x in range(nx):
        for core, part in enumerate(quads(got[:, 0, x], got[:, 1, x])):
            turned[core, x] = part.reshape(rows, wide)
    for core in range(cores):
        for x in range(nx):
            part = turned[core, x].astype(BF16)
            for c in range(copies):
                out_ref[core, c, x] = part


def up_kernel(rows_ref, gain_ref, weights_ref, out_ref, whole, normed):
    cores, pieces, part, wide = rows_ref.shape
    group = cores * part
    full = normed.shape[1]
    squares = [jnp.zeros((group, wide), F32) for _ in range(2)]
    for j in range(pieces // 2):
        even, odd = (
            jnp.concatenate([rows_ref[c, 2 * j + i].astype(F32) for c in range(cores)], 0)
            for i in range(2)
        )
        pair = halves(even, odd)
        for h in range(2):
            whole[h * group : (h + 1) * group, j * wide : (j + 1) * wide] = pair[h]
            squares[h] = squares[h] + pair[h] * pair[h]
    for h in range(2):
        mean = jnp.sum(squares[h], axis=1, keepdims=True) / full
        inverse = lax.rsqrt(mean + EPSILON)
        rows = slice(h * group, (h + 1) * group)
        normed[rows] = (whole[rows] * inverse * gain_ref[...]).astype(BF16)
    nx, _, units, _ = weights_ref.shape
    w_gate = weights_ref[:, 0].reshape(nx * units, full)
    w_up = weights_ref[:, 1].reshape(nx * units, full)
    gate = jnp.minimum(dot_nt(normed[...], w_gate), LIMIT)
    up = jnp.clip(dot_nt(normed[...], w_up), -LIMIT, LIMIT)
    hidden = ((up + 1.0) * gate * jax.nn.sigmoid(ALPHA * gate)).astype(BF16)
    for c in range(out_ref.shape[0]):
        out_ref[c] = hidden


def down_kernel(cores, hidden_ref, weights_ref, out_ref, turned):
    ny, rows, units = hidden_ref.shape
    nx, width, full = weights_ref.shape
    w_down = weights_ref[...].reshape(nx * width, full)
    total = dot_nt(hidden_ref[0], w_down[:, :units])
    for y in range(1, ny):
        total = total + dot_nt(hidden_ref[y], w_down[:, y * units : (y + 1) * units])
    group = rows // 2
    pieces = []
    for j in range(nx // 2):
        lanes = slice(2 * j * width, 2 * (j + 1) * width)
        pieces += halves(total[:group, lanes], total[group:, lanes])
    for j in range(nx // 2):
        first, second = (p.reshape(-1, 8, 2 * width) for p in pieces[2 * j : 2 * j + 2])
        for odd, part in enumerate(quads(first, second)):
            part = part.reshape(cores, -1, 8, 2 * width)
            for core in range(cores):
                turned[:, odd, core, j] = part[core]
    out_ref[...] = turned[...].reshape(out_ref.shape).astype(BF16)


def combine_kernel(back_ref, first_ref, rest_ref, out_ref):
    count = back_ref.shape[0]
    width = out_ref.shape[0]
    back = back_ref[...].astype(F32).T.astype(BF16)
    total = jnp.zeros(out_ref.shape, F32)
    for h in range(2):
        piece = back[h * width : (h + 1) * width]
        for part in (first_ref, rest_ref):
            total = total + dot(piece, part[h * count : (h + 1) * count])
    out_ref[...] = total.astype(BF16)


def call(kernel, out_shapes, *args, flops=1 << 24, scratch=(), space=pltpu.VMEM, vmem=16):
    single = not isinstance(out_shapes, list)
    outs = [out_shapes] if single else out_shapes
    out_specs = [pl.BlockSpec(memory_space=pltpu.VMEM)] * len(outs)
    return pl.pallas_call(
        kernel,
        out_shape=out_shapes,
        in_specs=[pl.BlockSpec(memory_space=space)] * len(args),
        out_specs=out_specs[0] if single else out_specs,
        scratch_shapes=list(scratch),
        cost_estimate=pl.CostEstimate(flops=flops, bytes_accessed=1 << 20, transcendentals=0),
        compiler_params=pltpu.CompilerParams(vmem_limit_bytes=vmem << 20),
    )(*args)


def set_at(whole, piece, index):
    return lax.dynamic_update_slice_in_dim(whole, piece[None], index, 0)


def gathered(shard, pair):
    count = lax.axis_size(TX)
    me = lax.axis_index(TX)
    near, far, after = (
        [(i, (i + hop) % count) for i in range(count)] for hop in (1, count - 2, count - 1)
    )
    right = lax.ppermute(shard, TX, after)
    across_pair = lax.ppermute(pair, TX, far)
    left = lax.ppermute(shard, TX, near)
    far_up = lax.ppermute(right[1], TX, after)
    up = jnp.zeros((count, 2) + shard.shape[1:], shard.dtype)
    down = jnp.zeros((count,) + shard.shape[1:], shard.dtype)
    before, behind, across = (lax.rem(me + hop, count) for hop in (count - 1, 1, count - 2))
    for piece, source in ((right, behind), (shard, me), (left, before)):
        up = set_at(up, piece[:2], source)
    for half, piece in enumerate((across_pair[0], far_up)):
        up = lax.dynamic_update_slice(up, piece[None, None], (across, half, 0, 0))
    for piece, source in ((right, behind), (left, before), (shard, me)):
        down = set_at(down, piece[2], source)
    down = set_at(down, across_pair[1], across)
    return up, down


def body(tokens, norm_gain, gate_weight, up_weight, down_weight, expert_ids, route_weight):
    tok_rows, top = expert_ids.shape
    width = tokens.shape[1]
    full = norm_gain.shape[0]
    nz, cores, ny, nx = (lax.axis_size(axis) for axis in (Z, CORE, TY, TX))
    ep, tp = nz * cores, ny * nx
    units = gate_weight.shape[2]
    half = tok_rows * top // ep
    inner = half // nx
    count, wide = ep * half, 2 * width
    group = count // nx
    shape = jax.ShapeDtypeStruct

    sent, place, shard, pair = call(
        functools.partial(prep_kernel, (nz, cores, nx)),
        [
            shape((count, wide), BF16),
            shape((top, tok_rows), I32),
            shape((3, units, full), BF16),
            shape((2, units, full), BF16),
        ],
        expert_ids.T,
        tokens.T,
        gate_weight[0].T,
        up_weight[0].T,
        down_weight[0].T,
        scratch=(
            pltpu.VMEM((top, tok_rows), I32),
            pltpu.VMEM((width, tok_rows), BF16),
            pltpu.SemaphoreType.DMA((7,)),
        ),
        space=pltpu.HBM,
        vmem=62,
    )
    got = lax.all_to_all(
        sent.reshape(nz * nx, cores * inner, wide), (Z, TX), 0, 0, tiled=True
    )
    w_up, w_down = gathered(shard, pair)

    spread = call(
        spread_kernel,
        shape((cores, ny, nx, nz * inner, wide), BF16),
        got.reshape(count, wide),
        scratch=(pltpu.VMEM((cores, nx, nz * inner, wide), F32),),
    )
    rows = lax.all_to_all(
        spread.reshape(cores * ny, nx * nz * inner, wide), (CORE, TY), 0, 0, tiled=True
    )
    first, rest, gain = call(
        mix_kernel,
        [shape((2 * count, tok_rows), BF16)] * 2 + [shape((1, full), F32)],
        place,
        route_weight.astype(F32).T,
        norm_gain.astype(F32).reshape(1, full),
    )
    hidden = call(
        up_kernel,
        shape((ny, 2 * group, nx * units), BF16),
        rows.reshape(cores, tp, nz * inner, wide),
        gain,
        w_up,
        flops=1 << 28,
        scratch=(pltpu.VMEM((2 * group, full), F32), pltpu.VMEM((2 * group, full), BF16)),
    )
    hidden = lax.all_to_all(hidden, TY, 0, 0, tiled=True)
    out = call(
        functools.partial(down_kernel, cores),
        shape((count, wide), BF16),
        hidden,
        w_down,
        flops=1 << 27,
        scratch=(pltpu.VMEM((nz // 2, 2, cores, nx // 2, 2 * inner, wide), F32),),
    )

    back = lax.all_to_all(
        out.reshape(ep * nx, inner, wide), (Z, CORE, TX), 0, 0, tiled=True
    )
    combined = call(
        combine_kernel, shape((width, tok_rows), BF16), back.reshape(count, wide), first, rest
    )
    return combined.T


def solution(mesh):
    devices = mesh.devices.reshape(mesh.shape["ep"] // 2, 2, 4, 4)
    split = Mesh(devices, (Z, CORE, TY, TX))
    in_specs = (
        P(EP, TP),
        P(),
        P(EP, None, TP),
        P(EP, None, TP),
        P(EP, None, TP),
        P(EP, None),
        P(EP, None),
    )
    return jax.shard_map(body, mesh=split, in_specs=in_specs, out_specs=P(EP, TP), check_vma=False)
```

```python
import functools

import jax
import jax.numpy as jnp
from jax import lax
from jax.experimental import pallas as pl
from jax.experimental.pallas import tpu as pltpu
from jax.sharding import Mesh
from jax.sharding import PartitionSpec as P


Z, CORE, TY, TX = "z", "core", "ty", "tx"
EP, TP = (Z, CORE), (TY, TX)
EPSILON = 1e-06
ALPHA = 1.702
LIMIT = 7.0
BF16, F32, I32 = jnp.bfloat16, jnp.float32, jnp.int32
NT = (((1,), (1,)), ((), ()))


def iota(shape, dim):
    return lax.broadcasted_iota(I32, shape, dim)


def dot(a, b):
    return jnp.dot(a, b, preferred_element_type=F32)


def dot_nt(a, b):
    return lax.dot_general(a, b, NT, preferred_element_type=F32)


def ones_where(mask):
    return jnp.where(mask, 1.0, 0.0).astype(BF16)


def quads(first, second):
    half = first.shape[1] // 2
    top = iota(first.shape, 1) < half
    return (
        jnp.where(top, first, pltpu.roll(second, half, 1)),
        jnp.where(top, pltpu.roll(first, half, 1), second),
    )


def halves(first, second):
    wide = first.shape[1] // 2
    left = iota(first.shape, 1) < wide
    return (
        jnp.where(left, first, pltpu.roll(second, wide, 1)),
        jnp.where(left, pltpu.roll(first, wide, 1), second),
    )


def prep_kernel(
    sizes, ids_hbm, tokens_hbm, gate_hbm, up_hbm, down_hbm, sent_ref, place_ref, shard_ref,
    ids_ref, tokens_ref, sems
):
    nz, cores, nx = sizes
    small = [(ids_hbm, ids_ref), (tokens_hbm, tokens_ref)]
    large = [(w, shard_ref.at[i]) for i, w in enumerate((gate_hbm, up_hbm, down_hbm))]
    copies = [pltpu.make_async_copy(a, b, sems.at[i]) for i, (a, b) in enumerate(small + large)]
    for copy in copies:
        copy.start()
    top, toks = ids_ref.shape
    count, _ = sent_ref.shape
    experts = nz * cores
    half = count // experts
    inner = half // nx
    earlier = ones_where(iota((toks, toks), 0) < iota((toks, toks), 1))
    expert = iota((experts, toks), 0)
    copies[0].wait()
    ids = ids_ref[...]
    picks = [expert == ids[k : k + 1] for k in range(top)]
    named = picks[0]
    for pick in picks[1:]:
        named = named | pick
    before = dot(ones_where(named), earlier)
    lane = iota((2 * count, toks), 0)
    hit = None
    for k in range(top):
        slot = jnp.sum(jnp.where(picks[k], before, 0.0), axis=0, keepdims=True).astype(I32)
        low, high = slot & (half - 1), jnp.where(slot >= half, count, 0)
        owner = ids[k : k + 1]
        place_ref[k : k + 1] = owner * half + low + high
        x, r = low >> (inner.bit_length() - 1), low & (inner - 1)
        z, core = owner >> (cores.bit_length() - 1), owner & (cores - 1)
        place = ((z * nx + x) * cores + core) * inner + r + high
        hit = (lane == place) if hit is None else hit | (lane == place)
    select = ones_where(hit)
    copies[1].wait()
    tokens = tokens_ref[...].astype(F32)
    zero = jnp.zeros_like(tokens)
    both = jnp.concatenate(
        [jnp.concatenate([tokens, zero], 1), jnp.concatenate([zero, tokens], 1)], 0
    ).astype(BF16)
    both_select = jnp.concatenate([select[:count], select[count:]], 1)
    sent_ref[...] = dot_nt(both_select, both).astype(BF16)
    for copy in copies[2:]:
        copy.wait()


def mix_kernel(place_ref, weight_ref, gain_ref, first_ref, rest_ref, gain_out_ref):
    gain_out_ref[...] = gain_ref[...]
    count, toks = first_ref.shape
    lane = iota((count, toks), 0)
    mix = jnp.zeros((count, toks), F32)
    for k in range(place_ref.shape[0]):
        mix = mix + jnp.where(lane == place_ref[k : k + 1], weight_ref[k : k + 1], 0.0)
    first = mix.astype(BF16)
    first_ref[...] = first
    rest_ref[...] = (mix - first.astype(F32)).astype(BF16)


def spread_kernel(got_ref, out_ref, turned):
    cores, copies, nx, rows, wide = out_ref.shape
    got = got_ref[...].astype(F32).reshape(-1, 2, nx, 8, wide)
    for x in range(nx):
        for core, part in enumerate(quads(got[:, 0, x], got[:, 1, x])):
            turned[core, x] = part.reshape(rows, wide)
    for core in range(cores):
        for x in range(nx):
            part = turned[core, x].astype(BF16)
            for c in range(copies):
                out_ref[core, c, x] = part


def norm_kernel(rows_ref, gain_ref, normed, whole):
    cores, pieces, part, wide = rows_ref.shape
    group = cores * part
    full = normed.shape[1]
    squares = [jnp.zeros((group, wide), F32) for _ in range(2)]
    for j in range(pieces // 2):
        even, odd = (
            jnp.concatenate([rows_ref[c, 2 * j + i].astype(F32) for c in range(cores)], 0)
            for i in range(2)
        )
        pair = halves(even, odd)
        for h in range(2):
            whole[h * group : (h + 1) * group, j * wide : (j + 1) * wide] = pair[h]
            squares[h] = squares[h] + pair[h] * pair[h]
    for h in range(2):
        mean = jnp.sum(squares[h], axis=1, keepdims=True) / full
        inverse = lax.rsqrt(mean + EPSILON)
        rows = slice(h * group, (h + 1) * group)
        normed[rows] = (whole[rows] * inverse * gain_ref[...]).astype(BF16)


def up_kernel(normed, weights_ref, out_ref):
    nx, _, units, full = weights_ref.shape
    w_gate = weights_ref[:, 0].reshape(nx * units, full)
    w_up = weights_ref[:, 1].reshape(nx * units, full)
    gate = jnp.minimum(dot_nt(normed[...], w_gate), LIMIT)
    up = jnp.clip(dot_nt(normed[...], w_up), -LIMIT, LIMIT)
    hidden = ((up + 1.0) * gate * jax.nn.sigmoid(ALPHA * gate)).astype(BF16)
    for c in range(out_ref.shape[0]):
        out_ref[c] = hidden


def down_kernel(cores, hidden_ref, weights_ref, out_ref, turned):
    ny, rows, units = hidden_ref.shape
    nx, width, full = weights_ref.shape
    w_down = weights_ref[...].reshape(nx * width, full)
    total = dot_nt(hidden_ref[0], w_down[:, :units])
    for y in range(1, ny):
        total = total + dot_nt(hidden_ref[y], w_down[:, y * units : (y + 1) * units])
    group = rows // 2
    pieces = []
    for j in range(nx // 2):
        lanes = slice(2 * j * width, 2 * (j + 1) * width)
        pieces += halves(total[:group, lanes], total[group:, lanes])
    for j in range(nx // 2):
        first, second = (p.reshape(-1, 8, 2 * width) for p in pieces[2 * j : 2 * j + 2])
        for odd, part in enumerate(quads(first, second)):
            part = part.reshape(cores, -1, 8, 2 * width)
            for core in range(cores):
                turned[:, odd, core, j] = part[core]
    out_ref[...] = turned[...].reshape(out_ref.shape).astype(BF16)


def combine_kernel(back_ref, first_ref, rest_ref, out_ref):
    count = back_ref.shape[0]
    width = out_ref.shape[0]
    back = back_ref[...].astype(F32).T.astype(BF16)
    total = jnp.zeros(out_ref.shape, F32)
    for h in range(2):
        piece = back[h * width : (h + 1) * width]
        for part in (first_ref, rest_ref):
            total = total + dot(piece, part[h * count : (h + 1) * count])
    out_ref[...] = total.astype(BF16)


def call(kernel, out_shapes, *args, flops=1 << 24, scratch=(), space=pltpu.VMEM, vmem=16):
    single = not isinstance(out_shapes, list)
    outs = [out_shapes] if single else out_shapes
    out_specs = [pl.BlockSpec(memory_space=pltpu.VMEM)] * len(outs)
    return pl.pallas_call(
        kernel,
        out_shape=out_shapes,
        in_specs=[pl.BlockSpec(memory_space=space)] * len(args),
        out_specs=out_specs[0] if single else out_specs,
        scratch_shapes=list(scratch),
        cost_estimate=pl.CostEstimate(flops=flops, bytes_accessed=1 << 20, transcendentals=0),
        compiler_params=pltpu.CompilerParams(vmem_limit_bytes=vmem << 20),
    )(*args)


def set_at(whole, piece, index):
    return lax.dynamic_update_slice_in_dim(whole, piece[None], index, 0)


def gathered(shard):
    count = lax.axis_size(TX)
    me = lax.axis_index(TX)
    near, after = ([(i, (i + hop) % count) for i in range(count)] for hop in (1, count - 1))
    left = lax.ppermute(shard, TX, near)
    right = lax.ppermute(shard, TX, after)
    far_up = lax.ppermute(left[:2], TX, near)
    far_down = lax.ppermute(right[2], TX, after)
    up = jnp.zeros((count, 2) + shard.shape[1:], shard.dtype)
    down = jnp.zeros((count,) + shard.shape[1:], shard.dtype)
    before, behind, across = (lax.rem(me + hop, count) for hop in (count - 1, 1, count - 2))
    for piece, source in ((left, before), (right, behind), (shard, me)):
        up = set_at(up, piece[:2], source)
    up = set_at(up, far_up, across)
    for piece, source in ((left, before), (right, behind), (shard, me)):
        down = set_at(down, piece[2], source)
    down = set_at(down, far_down, across)
    return up, down


def body(tokens, norm_gain, gate_weight, up_weight, down_weight, expert_ids, route_weight):
    tok_rows, top = expert_ids.shape
    width = tokens.shape[1]
    full = norm_gain.shape[0]
    nz, cores, ny, nx = (lax.axis_size(axis) for axis in (Z, CORE, TY, TX))
    ep, tp = nz * cores, ny * nx
    units = gate_weight.shape[2]
    half = tok_rows * top // ep
    inner = half // nx
    count, wide = ep * half, 2 * width
    group = count // nx
    shape = jax.ShapeDtypeStruct

    sent, place, shard = call(
        functools.partial(prep_kernel, (nz, cores, nx)),
        [
            shape((count, wide), BF16),
            shape((top, tok_rows), I32),
            shape((3, units, full), BF16),
        ],
        expert_ids.T,
        tokens.T,
        gate_weight[0].T,
        up_weight[0].T,
        down_weight[0].T,
        scratch=(
            pltpu.VMEM((top, tok_rows), I32),
            pltpu.VMEM((width, tok_rows), BF16),
            pltpu.SemaphoreType.DMA((5,)),
        ),
        space=pltpu.HBM,
        vmem=62,
    )
    got = lax.all_to_all(
        sent.reshape(nz * nx, cores * inner, wide), (Z, TX), 0, 0, tiled=True
    )
    w_up, w_down = gathered(shard)

    spread = call(
        spread_kernel,
        shape((cores, ny, nx, nz * inner, wide), BF16),
        got.reshape(count, wide),
        scratch=(pltpu.VMEM((cores, nx, nz * inner, wide), F32),),
    )
    rows = lax.all_to_all(
        spread.reshape(cores * ny, nx * nz * inner, wide), (CORE, TY), 0, 0, tiled=True
    )
    first, rest, gain = call(
        mix_kernel,
        [shape((2 * count, tok_rows), BF16)] * 2 + [shape((1, full), F32)],
        place,
        route_weight.astype(F32).T,
        norm_gain.astype(F32).reshape(1, full),
    )
    normed = call(
        norm_kernel,
        shape((2 * group, full), BF16),
        rows.reshape(cores, tp, nz * inner, wide),
        gain,
        scratch=(pltpu.VMEM((2 * group, full), F32),),
    )
    hidden = call(up_kernel, shape((ny, 2 * group, nx * units), BF16), normed, w_up, flops=1 << 28)
    hidden = lax.all_to_all(hidden, TY, 0, 0, tiled=True)
    out = call(
        functools.partial(down_kernel, cores),
        shape((count, wide), BF16),
        hidden,
        w_down,
        flops=1 << 27,
        scratch=(pltpu.VMEM((nz // 2, 2, cores, nx // 2, 2 * inner, wide), F32),),
    )

    back = lax.all_to_all(
        out.reshape(ep * nx, inner, wide), (Z, CORE, TX), 0, 0, tiled=True
    )
    combined = call(
        combine_kernel, shape((width, tok_rows), BF16), back.reshape(count, wide), first, rest
    )
    return combined.T


def solution(mesh):
    devices = mesh.devices.reshape(mesh.shape["ep"] // 2, 2, 4, 4)
    split = Mesh(devices, (Z, CORE, TY, TX))
    in_specs = (
        P(EP, TP),
        P(),
        P(EP, None, TP),
        P(EP, None, TP),
        P(EP, None, TP),
        P(EP, None),
        P(EP, None),
    )
    return jax.shard_map(body, mesh=split, in_specs=in_specs, out_specs=P(EP, TP), check_vma=False)
```

```python
import functools

import jax
import jax.numpy as jnp
from jax import lax
from jax.experimental import pallas as pl
from jax.experimental.pallas import tpu as pltpu
from jax.sharding import Mesh
from jax.sharding import PartitionSpec as P


Z, CORE, TY, TX = "z", "core", "ty", "tx"
EP, TP = (Z, CORE), (TY, TX)
EPSILON = 1e-06
ALPHA = 1.702
LIMIT = 7.0
BF16, F32, I32 = jnp.bfloat16, jnp.float32, jnp.int32
NT = (((1,), (1,)), ((), ()))


def iota(shape, dim):
    return lax.broadcasted_iota(I32, shape, dim)


def dot(a, b):
    return jnp.dot(a, b, preferred_element_type=F32)


def dot_nt(a, b):
    return lax.dot_general(a, b, NT, preferred_element_type=F32)


def ones_where(mask):
    return jnp.where(mask, 1.0, 0.0).astype(BF16)


def quads(first, second):
    half = first.shape[1] // 2
    top = iota(first.shape, 1) < half
    return (
        jnp.where(top, first, pltpu.roll(second, half, 1)),
        jnp.where(top, pltpu.roll(first, half, 1), second),
    )


def halves(first, second):
    wide = first.shape[1] // 2
    left = iota(first.shape, 1) < wide
    return (
        jnp.where(left, first, pltpu.roll(second, wide, 1)),
        jnp.where(left, pltpu.roll(first, wide, 1), second),
    )


def prep_kernel(
    sizes, ids_hbm, tokens_hbm, gate_hbm, up_hbm, down_hbm, sent_ref, place_ref, shard_ref,
    ids_ref, tokens_ref, sems
):
    nz, cores, nx = sizes
    small = [(ids_hbm, ids_ref), (tokens_hbm, tokens_ref)]
    large = [(w, shard_ref.at[i]) for i, w in enumerate((gate_hbm, up_hbm, down_hbm))]
    copies = [pltpu.make_async_copy(a, b, sems.at[i]) for i, (a, b) in enumerate(small + large)]
    for copy in copies:
        copy.start()
    top, toks = ids_ref.shape
    count, _ = sent_ref.shape
    experts = nz * cores
    half = count // experts
    inner = half // nx
    earlier = ones_where(iota((toks, toks), 0) < iota((toks, toks), 1))
    expert = iota((experts, toks), 0)
    copies[0].wait()
    ids = ids_ref[...]
    picks = [expert == ids[k : k + 1] for k in range(top)]
    named = picks[0]
    for pick in picks[1:]:
        named = named | pick
    before = dot(ones_where(named), earlier)
    lane = iota((2 * count, toks), 0)
    hit = None
    for k in range(top):
        slot = jnp.sum(jnp.where(picks[k], before, 0.0), axis=0, keepdims=True).astype(I32)
        low, high = slot & (half - 1), jnp.where(slot >= half, count, 0)
        owner = ids[k : k + 1]
        place_ref[k : k + 1] = owner * half + low + high
        x, r = low >> (inner.bit_length() - 1), low & (inner - 1)
        z, core = owner >> (cores.bit_length() - 1), owner & (cores - 1)
        place = ((z * nx + x) * cores + core) * inner + r + high
        hit = (lane == place) if hit is None else hit | (lane == place)
    select = ones_where(hit)
    copies[1].wait()
    tokens = tokens_ref[...].astype(F32)
    zero = jnp.zeros_like(tokens)
    both = jnp.concatenate(
        [jnp.concatenate([tokens, zero], 1), jnp.concatenate([zero, tokens], 1)], 0
    ).astype(BF16)
    both_select = jnp.concatenate([select[:count], select[count:]], 1)
    sent_ref[...] = dot_nt(both_select, both).astype(BF16)
    for copy in copies[2:]:
        copy.wait()


def mix_kernel(place_ref, weight_ref, gain_ref, first_ref, rest_ref, gain_out_ref):
    gain_out_ref[...] = gain_ref[...]
    count, toks = first_ref.shape
    lane = iota((count, toks), 0)
    mix = jnp.zeros((count, toks), F32)
    for k in range(place_ref.shape[0]):
        mix = mix + jnp.where(lane == place_ref[k : k + 1], weight_ref[k : k + 1], 0.0)
    first = mix.astype(BF16)
    first_ref[...] = first
    rest_ref[...] = (mix - first.astype(F32)).astype(BF16)


def spread_kernel(got_ref, out_ref, turned):
    cores, copies, nx, rows, wide = out_ref.shape
    got = got_ref[...].astype(F32).reshape(-1, 2, nx, 8, wide)
    for x in range(nx):
        for core, part in enumerate(quads(got[:, 0, x], got[:, 1, x])):
            turned[core, x] = part.reshape(rows, wide)
    for core in range(cores):
        for x in range(nx):
            part = turned[core, x].astype(BF16)
            for c in range(copies):
                out_ref[core, c, x] = part


def norm_kernel(rows_ref, gain_ref, normed, whole):
    cores, pieces, part, wide = rows_ref.shape
    group = cores * part
    full = normed.shape[1]
    squares = [jnp.zeros((group, wide), F32) for _ in range(2)]
    for j in range(pieces // 2):
        even, odd = (
            jnp.concatenate([rows_ref[c, 2 * j + i].astype(F32) for c in range(cores)], 0)
            for i in range(2)
        )
        pair = halves(even, odd)
        for h in range(2):
            whole[h * group : (h + 1) * group, j * wide : (j + 1) * wide] = pair[h]
            squares[h] = squares[h] + pair[h] * pair[h]
    for h in range(2):
        mean = jnp.sum(squares[h], axis=1, keepdims=True) / full
        inverse = lax.rsqrt(mean + EPSILON)
        rows = slice(h * group, (h + 1) * group)
        normed[rows] = (whole[rows] * inverse * gain_ref[...]).astype(BF16)


def up_kernel(normed, weights_ref, out_ref):
    nx, _, units, full = weights_ref.shape
    w_gate = weights_ref[:, 0].reshape(nx * units, full)
    w_up = weights_ref[:, 1].reshape(nx * units, full)
    gate = jnp.minimum(dot_nt(normed[...], w_gate), LIMIT)
    up = jnp.clip(dot_nt(normed[...], w_up), -LIMIT, LIMIT)
    hidden = ((up + 1.0) * gate * jax.nn.sigmoid(ALPHA * gate)).astype(BF16)
    for c in range(out_ref.shape[0]):
        out_ref[c] = hidden


def down_kernel(cores, hidden_ref, weights_ref, out_ref, turned):
    ny, rows, units = hidden_ref.shape
    nx, width, full = weights_ref.shape
    w_down = weights_ref[...].reshape(nx * width, full)
    total = dot_nt(hidden_ref[0], w_down[:, :units])
    for y in range(1, ny):
        total = total + dot_nt(hidden_ref[y], w_down[:, y * units : (y + 1) * units])
    group = rows // 2
    pieces = []
    for j in range(nx // 2):
        lanes = slice(2 * j * width, 2 * (j + 1) * width)
        pieces += halves(total[:group, lanes], total[group:, lanes])
    for j in range(nx // 2):
        first, second = (p.reshape(-1, 8, 2 * width) for p in pieces[2 * j : 2 * j + 2])
        for odd, part in enumerate(quads(first, second)):
            part = part.reshape(cores, -1, 8, 2 * width)
            for core in range(cores):
                turned[:, odd, core, j] = part[core]
    out_ref[...] = turned[...].reshape(out_ref.shape).astype(BF16)


def combine_kernel(back_ref, first_ref, rest_ref, out_ref):
    count = back_ref.shape[0]
    width = out_ref.shape[0]
    back = back_ref[...].astype(F32).T.astype(BF16)
    total = jnp.zeros(out_ref.shape, F32)
    for h in range(2):
        piece = back[h * width : (h + 1) * width]
        for part in (first_ref, rest_ref):
            total = total + dot(piece, part[h * count : (h + 1) * count])
    out_ref[...] = total.astype(BF16)


def call(kernel, out_shapes, *args, flops=1 << 24, scratch=(), space=pltpu.VMEM, vmem=16):
    single = not isinstance(out_shapes, list)
    outs = [out_shapes] if single else out_shapes
    out_specs = [pl.BlockSpec(memory_space=pltpu.VMEM)] * len(outs)
    return pl.pallas_call(
        kernel,
        out_shape=out_shapes,
        in_specs=[pl.BlockSpec(memory_space=space)] * len(args),
        out_specs=out_specs[0] if single else out_specs,
        scratch_shapes=list(scratch),
        cost_estimate=pl.CostEstimate(flops=flops, bytes_accessed=1 << 20, transcendentals=0),
        compiler_params=pltpu.CompilerParams(vmem_limit_bytes=vmem << 20),
    )(*args)


def set_at(whole, piece, index):
    return lax.dynamic_update_slice_in_dim(whole, piece[None], index, 0)


def gathered(shard):
    count = lax.axis_size(TX)
    me = lax.axis_index(TX)
    core = lax.axis_index(CORE)

    def hops(step):
        return [
            (c * count + i, c * count + (i + (step if c == 0 else -step)) % count)
            for c in range(lax.axis_size(CORE))
            for i in range(count)
        ]

    near, after, ring = hops(1), hops(-1), (CORE, TX)
    left = lax.ppermute(shard, ring, near)
    right = lax.ppermute(shard, ring, after)
    far_up = lax.ppermute(left[:2], ring, near)
    far_down = lax.ppermute(right[2], ring, after)
    up = jnp.zeros((count, 2) + shard.shape[1:], shard.dtype)
    down = jnp.zeros((count,) + shard.shape[1:], shard.dtype)
    one = jnp.where(core == 0, 1, count - 1)
    before, behind, across = (lax.rem(me + hop, count) for hop in (count - one, one, count - 2))
    for piece, source in ((left, before), (right, behind), (shard, me)):
        up = set_at(up, piece[:2], source)
    up = set_at(up, far_up, across)
    for piece, source in ((left, before), (shard, me), (right, behind)):
        down = set_at(down, piece[2], source)
    down = set_at(down, far_down, across)
    return up, down


def body(tokens, norm_gain, gate_weight, up_weight, down_weight, expert_ids, route_weight):
    tok_rows, top = expert_ids.shape
    width = tokens.shape[1]
    full = norm_gain.shape[0]
    nz, cores, ny, nx = (lax.axis_size(axis) for axis in (Z, CORE, TY, TX))
    ep, tp = nz * cores, ny * nx
    units = gate_weight.shape[2]
    half = tok_rows * top // ep
    inner = half // nx
    count, wide = ep * half, 2 * width
    group = count // nx
    shape = jax.ShapeDtypeStruct

    sent, place, shard = call(
        functools.partial(prep_kernel, (nz, cores, nx)),
        [
            shape((count, wide), BF16),
            shape((top, tok_rows), I32),
            shape((3, units, full), BF16),
        ],
        expert_ids.T,
        tokens.T,
        gate_weight[0].T,
        up_weight[0].T,
        down_weight[0].T,
        scratch=(
            pltpu.VMEM((top, tok_rows), I32),
            pltpu.VMEM((width, tok_rows), BF16),
            pltpu.SemaphoreType.DMA((5,)),
        ),
        space=pltpu.HBM,
        vmem=62,
    )
    got = lax.all_to_all(
        sent.reshape(nz * nx, cores * inner, wide), (Z, TX), 0, 0, tiled=True
    )
    w_up, w_down = gathered(shard)

    spread = call(
        spread_kernel,
        shape((cores, ny, nx, nz * inner, wide), BF16),
        got.reshape(count, wide),
        scratch=(pltpu.VMEM((cores, nx, nz * inner, wide), F32),),
    )
    rows = lax.all_to_all(
        spread.reshape(cores * ny, nx * nz * inner, wide), (CORE, TY), 0, 0, tiled=True
    )
    first, rest, gain = call(
        mix_kernel,
        [shape((2 * count, tok_rows), BF16)] * 2 + [shape((1, full), F32)],
        place,
        route_weight.astype(F32).T,
        norm_gain.astype(F32).reshape(1, full),
    )
    normed = call(
        norm_kernel,
        shape((2 * group, full), BF16),
        rows.reshape(cores, tp, nz * inner, wide),
        gain,
        scratch=(pltpu.VMEM((2 * group, full), F32),),
    )
    hidden = call(up_kernel, shape((ny, 2 * group, nx * units), BF16), normed, w_up, flops=1 << 28)
    hidden = lax.all_to_all(hidden, TY, 0, 0, tiled=True)
    out = call(
        functools.partial(down_kernel, cores),
        shape((count, wide), BF16),
        hidden,
        w_down,
        flops=1 << 27,
        scratch=(pltpu.VMEM((nz // 2, 2, cores, nx // 2, 2 * inner, wide), F32),),
    )

    back = lax.all_to_all(
        out.reshape(ep * nx, inner, wide), (Z, CORE, TX), 0, 0, tiled=True
    )
    combined = call(
        combine_kernel, shape((width, tok_rows), BF16), back.reshape(count, wide), first, rest
    )
    return combined.T


def solution(mesh):
    devices = mesh.devices.reshape(mesh.shape["ep"] // 2, 2, 4, 4)
    split = Mesh(devices, (Z, CORE, TY, TX))
    in_specs = (
        P(EP, TP),
        P(),
        P(EP, None, TP),
        P(EP, None, TP),
        P(EP, None, TP),
        P(EP, None),
        P(EP, None),
    )
    return jax.shard_map(body, mesh=split, in_specs=in_specs, out_specs=P(EP, TP), check_vma=False)
```
